32 devices in a mesh: ep: 8 (over z, y), tp: 4 (over x, core).
Axes of the slice: x: 2, y: 2, z: 4, core: 2. Of those that a mesh axis runs over, the one named last changes fastest.
Arguments:
- tokens: bfloat16 [2048, 2048], P('ep'), may hold values from -6 to 6
- norm_gain: float32 [2048], replicated, may hold values from 0.1 to 1.9
- expert_ids: int32 [2048, 2], P('ep'), may hold values from 0 to 3, all different within a row; in each aligned block of 256 rows (0 to 255, 256 to 511, ...) at most 160 rows name the same one
- route_weight: float32 [2048, 2], P('ep'), may hold values from 0.2 to 1
- w_gate: bfloat16 [8, 2048, 3584], P('ep', None, 'tp'), may hold values from -0.125 to 0.125
- w_up: bfloat16 [8, 2048, 3584], P('ep', None, 'tp'), may hold values from -0.125 to 0.125
- w_down: bfloat16 [8, 3584, 2048], P('ep', 'tp'), may hold values from -0.0625 to 0.0625
Outputs:
- mixed: bfloat16 [2048, 2048], P('ep', 'tp')
The draws below stay inside these ranges and needn't reach their ends.
Inputs may be any that keep to these rules, and one draw needn't show every extreme that they name: `expert_ids`: A token names 2 different experts. In each aligned block of 256 tokens (the tokens of one index of ep) no expert is named by more than 160 tokens, a bound that some block reaches.
All inputs are finite; a program needn't handle non-finite values.
Results may differ from the reference program's by a relative error of at most 0.014.
Values may be sent and summed in bfloat16 or wider, within the bound.
A program may use at most 128 MiB of HBM per device.

```python
import math
import jax
import jax.numpy as jnp
import numpy as np
from jax import lax

D = 2048
FF = 7168
TOP = 2
HALVES = 2
TOK_DEV = 256
EXPERTS = 4
HALF_FF = 3584
BLOCK_H = 896
CAP = 160
TOKENS = 2048
N_EP = 8
N_TP = 4


def steps_of(key, dims, pieces, smallest, top_value):
    loudness = 1.0
    for axis_at, shards_of in pieces:
        heights = jax.random.uniform(jax.random.fold_in(jax.random.fold_in(key, 6), axis_at), (shards_of,), jnp.float32, smallest / len(pieces), top_value / len(pieces))
        loudness = loudness * jnp.repeat(jnp.exp(heights), dims[axis_at] // shards_of).reshape((-1,) + (1,) * (len(dims) - 1 - axis_at))
    return loudness


def assign_block(rng, own, number, rows, number_of, top, bound, slope):
    sequence = jax.random.permutation(rng, number_of)
    packed, ordinary = shares(number_of, rows * top, bound, slope, True), shares(number_of, rows * top, bound, slope, False)
    places = jnp.arange(number_of)

    def named(tallies, offset_by):
        used = int((tallies > 0).sum())
        fixed = max(1, used // 4)
        shifted = fixed + (places - fixed + offset_by * (used - fixed)) % max(1, number_of - fixed)
        return jnp.zeros((number_of,), jnp.int32).at[sequence[jnp.where(places < fixed, places, shifted)]].set(jnp.asarray(tallies, jnp.int32))

    tallies = jnp.where(number % 4 == 0, named(packed, number // 4), named(ordinary, number - number // 4 - 1))
    mixed = jax.random.permutation(jax.random.fold_in(own, 3), number_of)
    donor, receiver = mixed[0:number_of // 2 * 2:2], mixed[1:number_of // 2 * 2:2]
    room = jnp.minimum(tallies[donor] - 1, bound - tallies[receiver]) // 2
    room = jnp.where((donor == sequence[0]) | (receiver == sequence[0]) | (tallies[receiver] == 0), 0, jnp.maximum(room, 0))
    shifted = jax.random.randint(jax.random.fold_in(own, 4), (number_of // 2,), 0, 1 << 20) % (room + 1)
    tallies = tallies.at[donor].add(-shifted).at[receiver].add(shifted)
    members = jnp.searchsorted(jnp.cumsum(tallies), jnp.arange(rows * top), side="right").astype(jnp.int32)
    table = members.reshape(top, rows).T
    table = table[jax.random.permutation(jax.random.fold_in(own, 1), rows)]
    offset_by = jax.random.randint(jax.random.fold_in(own, 2), (rows, 1), 0, top)
    return jnp.take_along_axis(table, (jnp.arange(top)[None, :] + offset_by) % top, axis=1)


def shares(count, total, reach, skew, full):
    portions = [(1 << 20) // math.isqrt(grade ** skew) + 1 for grade in range(1, count + 1)]
    largest = reach if full else min(reach, max(-(-total // count), total * portions[0] // sum(portions)))
    least = 1 if total - largest >= count - 1 else 0
    holding, surplus = [largest] + [least] * (count - 1), total - largest - least * (count - 1)
    while surplus > 0:
        movable = [i for i in range(1, count) if holding[i] < largest] or [i for i in range(1, count) if holding[i] < reach]
        mass, remaining = sum([portions[i] for i in movable]), surplus
        for i in movable:
            addition = min(reach - holding[i], max(1, remaining * portions[i] // mass), surplus)
            holding[i] = holding[i] + addition
            surplus = surplus - addition
    return np.array(holding)


def normal_values(own_key, extent, scale, most, split=(), kind=jnp.bfloat16):
    gain = steps_of(own_key, extent, split, -0.22, 0.18) if split else 1.0
    entries = jax.random.normal(own_key, extent, jnp.float32) * scale * gain
    return jnp.minimum(jnp.maximum(entries, -most), most).astype(kind)


def setup_inputs(seed: int = 0) -> dict:
    key_list = jax.random.split(jax.random.key(seed), 8)
    tokens = normal_values(key_list[0], (TOKENS, D), 1.0, 6.0, ((0, 8),))
    norm_gain = jnp.clip(1.0 + 0.18 * jax.random.normal(key_list[1], (D,), jnp.float32), 0.1, 1.9)
    expert_ids_keys = jax.random.split(jax.random.fold_in(key_list[2], 1), TOKENS // TOK_DEV)
    expert_ids_turns = jax.random.permutation(jax.random.fold_in(key_list[2], 3), TOKENS // TOK_DEV)
    expert_ids = jax.vmap(lambda own, number: assign_block(jax.random.fold_in(key_list[2], 2), own, number, TOK_DEV, EXPERTS, TOP, CAP, 1))(expert_ids_keys, expert_ids_turns).reshape((TOKENS, TOP))
    route_weight = jnp.clip(0.2 + 0.8 * jax.random.uniform(key_list[3], (TOKENS, TOP), jnp.float32) ** steps_of(key_list[3], (TOKENS, TOP), ((0, 8),), -0.2, 0.2), 0.2, 1.0)
    w_gate = normal_values(key_list[4], (EXPERTS * HALVES, D, HALF_FF), D ** -0.5, 0.125, ((0, 8), (2, 4)))
    w_up = normal_values(key_list[5], (EXPERTS * HALVES, D, HALF_FF), D ** -0.5, 0.125, ((0, 8), (2, 4)))
    w_down = normal_values(key_list[6], (EXPERTS * HALVES, HALF_FF, D), FF ** -0.5, 0.0625, ((0, 8), (1, 4)))
    return {"tokens": tokens, "norm_gain": norm_gain, "expert_ids": expert_ids, "route_weight": route_weight, "w_gate": w_gate, "w_up": w_up, "w_down": w_down}


EPSILON = 1e-05

def layer_normed(tokens, norm_gain):
    values = tokens.astype(jnp.float32)
    center = values - lax.optimization_barrier(jnp.mean(values, axis=-1, keepdims=True))
    spread = lax.optimization_barrier(jnp.mean(center * center, axis=-1, keepdims=True))
    return (center * lax.rsqrt(spread + EPSILON) * norm_gain).astype(jnp.bfloat16)

def slot_numbers(chosen, experts):
    onehot = (chosen[..., None] == jnp.arange(experts, dtype=jnp.int32)).astype(jnp.int32)
    before = jnp.cumsum(onehot, axis=1) - onehot
    return lax.optimization_barrier(jnp.sum(before * onehot, axis=-1)).astype(jnp.int32)

def reference(tokens, norm_gain, expert_ids, route_weight, w_gate, w_up, w_down):
    normed = layer_normed(tokens, norm_gain)
    padded = jnp.concatenate([normed, jnp.zeros((1, D), jnp.bfloat16)], axis=0)
    pair_count = TOK_DEV * TOP
    slots = slot_numbers(expert_ids.reshape(N_EP, pair_count), EXPERTS).reshape(-1)
    flat_expert = expert_ids.reshape(-1).astype(jnp.int32)
    index = jnp.arange(TOKENS * TOP, dtype=jnp.int32)
    source = index // pair_count
    owner = index // TOP
    place = (flat_expert * N_EP + source) * CAP + slots
    table = jnp.full((EXPERTS * N_EP * CAP,), TOKENS, jnp.int32).at[place].set(owner)
    table = table.reshape(EXPERTS, N_EP * CAP)

    def one_expert(expert):
        rows = padded[table[expert]]
        total = jnp.zeros((N_EP * CAP, D), jnp.float32)
        for half in range(HALVES):
            which = expert * HALVES + half
            gate = jnp.dot(rows, w_gate[which], preferred_element_type=jnp.float32)
            up = jnp.dot(rows, w_up[which], preferred_element_type=jnp.float32)
            hidden = (jax.nn.silu(gate) * up).astype(jnp.bfloat16)
            blocks = hidden.reshape(N_EP * CAP, N_TP, BLOCK_H).astype(jnp.float32)
            down = w_down[which].reshape(N_TP, BLOCK_H, D).astype(jnp.float32)
            block_out = jnp.einsum('rnb,nbd->nrd', blocks, down).astype(jnp.bfloat16)
            half_out = lax.optimization_barrier(jnp.sum(block_out.astype(jnp.float32), axis=0)).astype(jnp.bfloat16)
            total = total + half_out.astype(jnp.float32)
        return total
    results = lax.map(one_expert, jnp.arange(EXPERTS, dtype=jnp.int32))
    merged = results.reshape(EXPERTS * N_EP * CAP, D)
    picked = merged[place].reshape(TOKENS, TOP, D)
    return lax.optimization_barrier(jnp.sum(route_weight[:, :, None] * picked, axis=1)).astype(jnp.bfloat16)
```

```python
import functools

import jax
import jax.numpy as jnp
from jax import lax
from jax.experimental import pallas as pl
from jax.experimental.pallas import tpu as pltpu
from jax.sharding import PartitionSpec as P

HALVES = 2
CORES = 2
EPSILON = 1e-05
MESH = pl.DeviceIdType.MESH
ORDER = (
    ('own_rest',),
    ('join', 0),
    ('expand', 0, 0),
    ('join', 1),
    ('launch', 1),
    ('launch', 2),
    ('expand', 0, 1),
    ('relay', 1),
    ('launch', 3),
    ('share', 1),
    ('shrink', 0, (1,)),
    ('finish', 1),
    ('relay', 2),
    ('expand', 1, 0),
    ('relay', 3),
    ('expand', 1, 1),
    ('shrink', 0, (0,)),
    ('shrink', 0, (2,)),
    ('shrink', 1, (0,)),
    ('share', 3),
    ('shrink', 1, (3,)),
    ('shrink', 1, (2,)),
    ('finish', 3),
    ('share', 2),
    ('expand', 3, 0),
    ('expand', 3, 1),
    ('shrink', 1, (1,)),
    ('second', 1),
    ('expand', 2, 0),
    ('shrink', 3, (3,)),
    ('finish', 2),
    ('shrink', 3, (1,)),
    ('shrink', 3, (2,)),
    ('third', 1),
    ('expand', 2, 1),
    ('second', 3),
    ('shrink', 3, (0,)),
    ('shrink', 2, (2,)),
    ('shrink', 2, (3,)),
    ('shrink', 2, (1,)),
    ('third', 3),
    ('shrink', 0, (3,)),
    ('shrink', 2, (0,)),
    ('second', 2),
    ('mix', 1),
    ('second', 0),
    ('third', 2),
    ('mix', 3),
    ('third', 0),
    ('mix', 0),
    ('mix', 2),
)
PARTNERS = ((2, 1, 3), (3, 0, 2))
MIXES = (1, 3, 0, 2)


def layer_normed(tokens, norm_gain):
    values = tokens.astype(jnp.float32)
    center = values - jnp.mean(values, axis=-1, keepdims=True)
    spread = jnp.mean(center * center, axis=-1, keepdims=True)
    return (center * lax.rsqrt(spread + EPSILON) * norm_gain).astype(jnp.bfloat16)


def slot_numbers(chosen, experts):
    onehot = (chosen[..., None] == jnp.arange(experts, dtype=jnp.int32)).astype(jnp.int32)
    before = jnp.cumsum(onehot, axis=1) - onehot
    return jnp.sum(before * onehot, axis=-1)


def capacity_of(tok_rows, top_count, experts):
    return 2 * min(tok_rows // 2, 5 * tok_rows * top_count // (8 * experts))


def kernel(experts, cap, tokens_ref, gain_ref, ids_ref, weight_ref, wg_hbm, wu_hbm, wd_hbm,
           out_hbm, wgu, wdc, out_ref, normed, picks, routed, away, hid, chip, hop1, turn, hop2, final, back, total,
           load_sem, ws, wr, zs, zr, as_, ar, ams, amr, xs, xr, fs, fr, ds, dr, hs, hr,
           h1s, h1r, h2s, h2r, bs, br):
    ep, tp = lax.axis_index("ep"), lax.axis_index("tp")
    z, y = ep // HALVES, ep % HALVES
    x, c = tp // CORES, tp % CORES
    tok_rows, width = tokens_ref.shape
    quarter = out_ref.shape[1]
    units = wdc.shape[0] // CORES
    bf16, f32 = jnp.bfloat16, jnp.float32

    def columns_of(xx, cc):
        return pl.ds(pl.multiple_of((xx * CORES + cc) * quarter, quarter), quarter)

    def rows_of(yy):
        return pl.ds(pl.multiple_of(yy * cap, cap), cap)

    own_units, mate_units = pl.ds(0, units), pl.ds(units, units)
    loads = [
        pltpu.make_async_copy(wg_hbm.at[0], wgu.at[:, own_units], load_sem.at[0]),
        pltpu.make_async_copy(wu_hbm.at[0], wgu.at[:, mate_units], load_sem.at[1]),
    ] + [
        pltpu.make_async_copy(
            wd_hbm.at[0, :, columns_of(xx, c)], wdc.at[own_units, pl.ds(xx * quarter, quarter)], load_sem.at[2 + xx]
        )
        for xx in range(2)
    ]
    for load in loads:
        load.start()

    def device(zz, yy, xx, cc):
        return (zz * HALVES + yy, xx * CORES + cc)

    x_peer = device(z, y, 1 - x, c)
    y_peer = device(z, 1 - y, x, c)
    mate_peer = device(z, y, x, 1 - c)
    first = (z * HALVES + (c * (1 - y) + (1 - c) * y), (c * x + (1 - c) * (1 - x)) * CORES + c)
    second = (z * HALVES + (c * y + (1 - c) * (1 - y)), (c * (1 - x) + (1 - c) * x) * CORES + c)

    plane = [z] + [nearest(z, k, experts) for k in range(experts - 1)]

    barrier = pltpu.get_barrier_semaphore()
    peers = [x_peer, y_peer, mate_peer] + [device(p, y, x, c) for p in plane[1:]]
    for peer in peers:
        pl.semaphore_signal(barrier, inc=1, device_id=peer, device_id_type=MESH)

    ids = jnp.transpose(ids_ref[...])
    one, two = ids[:, 0:1], ids[:, 1:2]
    lane = lax.broadcasted_iota(jnp.int32, (tok_rows, 128), 1)
    places = lax.broadcasted_iota(jnp.int32, (tok_rows, cap), 1)
    expert = jnp.full((tok_rows, 128), -1, jnp.int32)
    for k, p in enumerate(plane):
        expert = jnp.where(lane == k, p, expert)
    named = jnp.logical_or(one == expert, two == expert)
    lower = (
        lax.broadcasted_iota(jnp.int32, (tok_rows, tok_rows), 1)
        < lax.broadcasted_iota(jnp.int32, (tok_rows, tok_rows), 0)
    )
    slot = jnp.dot(
        lower.astype(f32).astype(bf16), named.astype(f32).astype(bf16), preferred_element_type=f32
    )
    slot = jnp.where(named, slot, -1.0).astype(jnp.int32)

    values = tokens_ref[...].astype(f32)
    mean = jnp.mean(values, axis=-1, keepdims=True)
    center = values - mean
    spread = jnp.mean(center * center, axis=-1, keepdims=True)
    scale = lax.rsqrt(spread + EPSILON)

    def norm(columns):
        own = tokens_ref[:, columns].astype(f32) - mean
        normed[:, columns] = (own * scale * gain_ref[:, columns]).astype(bf16)

    def pick(k, columns):
        return lax.dot_general(
            picks[k], normed[:, columns], (((0,), (0,)), ((), ())), preferred_element_type=f32
        ).astype(bf16)

    mine = columns_of(x, c)
    norm(mine)
    for k in range(1, experts):
        picks[k] = (places == slot[:, k:k + 1]).astype(f32).astype(bf16)
        away[k - 1] = pick(k, mine)
    picks[0] = (places == slot[:, 0:1]).astype(f32).astype(bf16)
    here = routed.at[z, rows_of(y)]
    here[:, mine] = pick(0, mine)
    norm(columns_of(1 - x, c))
    here[:, columns_of(1 - x, c)] = pick(0, columns_of(1 - x, c))

    sent = []

    def send(src, dst, send_sem, recv_sem, peer):
        copy = pltpu.make_async_remote_copy(
            src_ref=src, dst_ref=dst, send_sem=send_sem, recv_sem=recv_sem,
            device_id=peer, device_id_type=MESH,
        )
        copy.start()
        sent.append(copy)
        return copy

    def block(p, yy, xx, cc):
        return routed.at[plane[p], rows_of(yy), columns_of(xx, cc)]

    pl.semaphore_wait(barrier, len(peers))
    for k in range(1, experts):
        send(away.at[k - 1], routed.at[z, rows_of(y), mine], zs.at[k - 1], zr.at[z], device(plane[k], y, x, c))
    for i, xx in enumerate((x, 1 - x)):
        b = block(0, y, xx, c)
        send(b, b, as_.at[i], ar.at[i], y_peer)
    w_copies = [
        send(wd_hbm.at[0, :, columns_of(xx, 1 - c)], wdc.at[mate_units, pl.ds(xx * quarter, quarter)],
             ws.at[xx], wr.at[xx], mate_peer)
        for xx in range(2)
    ]

    def arrived(dst, sem):
        pltpu.make_async_remote_copy(
            src_ref=dst, dst_ref=dst, send_sem=zs.at[0], recv_sem=sem,
            device_id=mate_peer, device_id_type=MESH,
        ).wait_recv()

    handed, ready = {}, set()
    hop1_copies, hop2_copies = {}, {}

    def own_rest():
        for xx in (x, 1 - x):
            columns = columns_of(xx, 1 - c)
            norm(columns)
            here[:, columns] = pick(0, columns)

    def join(i):
        xx = 1 - x if i else x
        b = block(0, 1 - y, xx, c)
        arrived(b, ar.at[i])
        send(b, b, ams.at[i], amr.at[i], mate_peer)

    def launch(p):
        b = block(p, y, x, c)
        arrived(b, zr.at[plane[p]])
        send(b, b, xs.at[p, 0], xr.at[p, 0], x_peer)
        send(b, b, xs.at[p, 1], xr.at[p, 1], y_peer)
        send(b, b, ds.at[p, 0], dr.at[p, 0], mate_peer)

    def relay(p):
        b = block(p, c * y + (1 - c) * (1 - y), c * (1 - x) + (1 - c) * x, c)
        arrived(b, xr.at[p, 1 - c])
        send(b, b, fs.at[p], fr.at[p], first)
        send(b, b, ds.at[p, 2 - c], dr.at[p, 2 - c], mate_peer)

    def share(p):
        b = block(p, (1 - c) * y + c * (1 - y), (1 - c) * (1 - x) + c * x, c)
        arrived(b, xr.at[p, c])
        send(b, b, ds.at[p, 1 + c], dr.at[p, 1 + c], mate_peer)

    def finish(p):
        b = block(p, 1 - y, 1 - x, c)
        arrived(b, fr.at[p])
        send(b, b, ds.at[p, 3], dr.at[p, 3], mate_peer)

    def expand(p, i):
        if p == 0 and i == 0:
            loads[0].wait()
            loads[1].wait()
        rows = rows_of(1 - y if i else y)
        if p == 0 and i == 1:
            arrived(block(0, 1 - y, x, 1 - c), amr.at[0])
            arrived(block(0, 1 - y, 1 - x, 1 - c), amr.at[1])
        elif p and i == 0:
            arrived(block(p, y, x, 1 - c), dr.at[p, 0])
            arrived(block(p, y, 1 - x, 1 - c), dr.at[p, 1])
        elif p:
            arrived(block(p, 1 - y, x, 1 - c), dr.at[p, 2])
            arrived(block(p, 1 - y, 1 - x, 1 - c), dr.at[p, 3])
        both = jnp.dot(routed[plane[p], rows], wgu[...], preferred_element_type=f32)
        gate, up = both[:, :units], both[:, units:]
        hid[p, rows, own_units] = (gate / (1.0 + jnp.exp(-gate)) * up).astype(bf16)
        handed[p, i] = send(
            hid.at[p, rows, own_units], hid.at[p, rows, mate_units], hs.at[p, i], hr.at[p, i], mate_peer
        )

    def shrink(p, js):
        if not ready:
            for copy in loads[2:]:
                copy.wait()
            for copy in w_copies:
                copy.wait_recv()
        if p not in ready:
            ready.add(p)
            for i in range(2):
                handed[p, i].wait_recv()
        for j in js:
            low, high = j % 2, j // 2
            x_low, x_high = (1 - x if low else x), (1 - x if high else x)
            y_low, y_high = (1 - y if low else y), (1 - y if high else y)
            xx = c * x_low + (1 - c) * x_high
            yy = c * y_high + (1 - c) * y_low
            chip[p, j] = jnp.dot(
                hid[p, rows_of(yy)], wdc[:, pl.ds(pl.multiple_of(xx * quarter, quarter), quarter)],
                preferred_element_type=f32,
            ).astype(bf16)
            if j >= 2:
                hop1_copies[p, j - 2] = send(
                    chip.at[p, j], hop1.at[p, j - 2], h1s.at[p, j - 2], h1r.at[p, j - 2], first
                )

    def return_second(p):
        hop1_copies[p, 1].wait_recv()
        turn[p] = (chip[p, 1].astype(f32) + hop1[p, 1].astype(f32)).astype(bf16)
        hop2_copies[p] = send(turn.at[p], hop2.at[p], h2s.at[p], h2r.at[p], second)

    def return_third(p):
        hop1_copies[p, 0].wait_recv()
        part = chip[p, 0].astype(f32) + hop1[p, 0].astype(f32)
        hop2_copies[p].wait_recv()
        part = (part + hop2[p].astype(f32)).astype(bf16)
        if p == 0:
            back[z] = part
        else:
            final[p - 1] = part
            send(final.at[p - 1], back.at[z], bs.at[p - 1], br.at[z], device(plane[p], y, x, c))

    def mix(p):
        e = plane[p]
        if p:
            arrived(back.at[e], br.at[e])
        route = jnp.transpose(weight_ref[...])
        share = jnp.where(one == e, route[:, 0:1], 0.0) + jnp.where(two == e, route[:, 1:2], 0.0)
        value = share * jnp.dot(picks[p], back[e], preferred_element_type=f32)
        if p == MIXES[0]:
            total[...] = value
        elif p != MIXES[-1]:
            total[...] += value
        else:
            out_ref[...] = (total[...] + value).astype(bf16)

    steps = dict(own_rest=own_rest, join=join, launch=launch, relay=relay, share=share, finish=finish, expand=expand,
                 shrink=shrink, second=return_second, third=return_third, mix=mix)
    for name, *arguments in ORDER:
        steps[name](*arguments)

    store = pltpu.make_async_copy(out_ref, out_hbm, load_sem.at[4])
    store.start()
    for copy in sent:
        copy.wait_send()
    store.wait()


def nearest(z, k, experts):
    place = 0
    for zz in range(experts):
        near = zz if zz < experts - 1 - zz else experts - 1 - zz
        other = PARTNERS[near][k]
        place = place + jnp.where(z == zz, other if near == zz else experts - 1 - other, 0)
    return place


def fused_body(tokens, norm_gain, expert_ids, route_weight, w_gate, w_up, w_down):
    tok_rows, width = tokens.shape
    experts = lax.axis_size("ep") // HALVES
    cap = capacity_of(tok_rows, expert_ids.shape[1], experts)
    tp_count = lax.axis_size("tp")
    quarter = width // tp_count
    units = w_gate.shape[2]
    bf16 = jnp.bfloat16
    dma = pltpu.SemaphoreType.DMA
    vmem = pl.BlockSpec(memory_space=pltpu.VMEM)
    hbm = pl.BlockSpec(memory_space=pl.ANY)
    one, two = dma((experts,)), dma((experts, 2))
    return pl.pallas_call(
        functools.partial(kernel, experts, cap),
        out_shape=jax.ShapeDtypeStruct((tok_rows, quarter), bf16),
        in_specs=[vmem, vmem, vmem, vmem, hbm, hbm, hbm],
        out_specs=hbm,
        scratch_shapes=[
            pltpu.VMEM((width, 2 * units), bf16),
            pltpu.VMEM((CORES * units, 2 * quarter), bf16),
            pltpu.VMEM((tok_rows, quarter), bf16),
            pltpu.VMEM((tok_rows, width), bf16),
            pltpu.VMEM((experts, tok_rows, cap), bf16),
            pltpu.VMEM((experts, HALVES * cap, width), bf16),
            pltpu.VMEM((experts - 1, cap, quarter), bf16),
            pltpu.VMEM((experts, HALVES * cap, CORES * units), bf16),
            pltpu.VMEM((experts, 4, cap, quarter), bf16),
            pltpu.VMEM((experts, 2, cap, quarter), bf16),
            pltpu.VMEM((experts, cap, quarter), bf16),
            pltpu.VMEM((experts, cap, quarter), bf16),
            pltpu.VMEM((experts - 1, cap, quarter), bf16),
            pltpu.VMEM((experts, cap, quarter), bf16),
            pltpu.VMEM((tok_rows, quarter), jnp.float32),
            dma((5,)),
            dma((2,)), dma((2,)),
            one, one,
            dma((2,)), dma((2,)), dma((2,)), dma((2,)),
            two, two, one, one,
            dma((experts, 4)), dma((experts, 4)),
            two, two,
            two, two, one, one, one, one,
        ],
        compiler_params=pltpu.CompilerParams(
            collective_id=0, has_side_effects=True, vmem_limit_bytes=60 * 1024 * 1024
        ),
        name="expert_layer",
    )(tokens, norm_gain.reshape(1, -1), expert_ids.T, route_weight.T, w_gate, w_up, w_down)


def body(tokens, norm_gain, expert_ids, route_weight, w_gate, w_up, w_down):
    tok_rows, width = tokens.shape
    top_count = expert_ids.shape[1]
    ep_count = lax.axis_size("ep")
    experts = ep_count // HALVES
    capacity = capacity_of(tok_rows, top_count, experts)
    normed = layer_normed(tokens, norm_gain)
    padded = jnp.concatenate([normed, jnp.zeros((1, width), jnp.bfloat16)], axis=0)
    slots = slot_numbers(expert_ids.reshape(1, -1), experts).reshape(-1)
    flat_expert = expert_ids.reshape(-1)
    owner = jnp.arange(tok_rows * top_count, dtype=jnp.int32) // top_count
    place = flat_expert * capacity + slots
    table = jnp.full((experts * capacity,), tok_rows, jnp.int32).at[place].set(owner)
    outgoing = padded[table].reshape(experts, capacity, width)
    columns = width // lax.axis_size("tp")
    portion = lax.dynamic_slice_in_dim(outgoing, lax.axis_index("tp") * columns, columns, 2)
    doubled = jnp.repeat(portion, HALVES, axis=0)
    pieces = lax.all_to_all(doubled, "ep", split_axis=0, concat_axis=0, tiled=True)
    arrived = lax.all_gather(pieces, "tp", axis=2, tiled=True)
    routed = arrived.reshape(-1, width)
    gate = jnp.dot(routed, w_gate[0], preferred_element_type=jnp.float32)
    up = jnp.dot(routed, w_up[0], preferred_element_type=jnp.float32)
    hidden = (jax.nn.silu(gate) * up).astype(jnp.bfloat16)
    partial_value = jnp.dot(hidden, w_down[0], preferred_element_type=jnp.float32)
    reduced = lax.psum_scatter(
        partial_value.astype(jnp.bfloat16), "tp", scatter_dimension=1, tiled=True
    )
    returned = lax.all_to_all(
        reduced.reshape(ep_count, capacity, -1), "ep", split_axis=0, concat_axis=0, tiled=True
    )
    quarter = returned.shape[2]
    summed = returned.reshape(experts, HALVES, capacity, quarter).astype(jnp.float32).sum(axis=1)
    picked = summed.reshape(experts * capacity, quarter)[place].reshape(
        tok_rows, top_count, quarter
    )
    mixed = jnp.sum(route_weight[:, :, None] * picked, axis=1)
    return mixed.astype(jnp.bfloat16)


def choose(*args):
    tok_rows = args[0].shape[0]
    experts = lax.axis_size("ep") // HALVES
    cap = capacity_of(tok_rows, args[2].shape[1], experts)
    if experts == len(MIXES) and cap % 16 == 0 and lax.axis_size("tp") == 2 * CORES and args[2].shape[1] == 2:
        return fused_body(*args)
    return body(*args)


def solution(mesh):
    return jax.shard_map(
        choose,
        mesh=mesh,
        in_specs=(
            P("ep", None),
            P(),
            P("ep", None),
            P("ep", None),
            P("ep", None, "tp"),
            P("ep", None, "tp"),
            P("ep", "tp", None),
        ),
        out_specs=P("ep", "tp"),
        check_vma=False,
    )
```

```python
import functools

import jax
import jax.numpy as jnp
from jax import lax
from jax.experimental import pallas as pl
from jax.experimental.pallas import tpu as pltpu
from jax.sharding import PartitionSpec as P

HALVES = 2
CORES = 2
EPSILON = 1e-05
MESH = pl.DeviceIdType.MESH
ORDER = (
    ('join', 0),
    ('own_rest',),
    ('launch', 1),
    ('join', 1),
    ('wsend',),
    ('expand', 0, 0),
    ('launch', 2),
    ('expand', 0, 1),
    ('relay', 1),
    ('share', 1),
    ('expand', 1, 0),
    ('launch', 3),
    ('finish', 1),
    ('shrink', 0, (0,)),
    ('relay', 2),
    ('share', 2),
    ('expand', 1, 1),
    ('share', 3),
    ('relay', 3),
    ('shrink', 1, (3,)),
    ('shrink', 1, (2,)),
    ('expand', 3, 0),
    ('shrink', 1, (1,)),
    ('finish', 2),
    ('finish', 3),
    ('expand', 2, 0),
    ('second', 1),
    ('expand', 3, 1),
    ('shrink', 0, (3,)),
    ('shrink', 1, (0,)),
    ('shrink', 3, (3,)),
    ('third', 1),
    ('shrink', 3, (2,)),
    ('shrink', 3, (1,)),
    ('shrink', 0, (1,)),
    ('expand', 2, 1),
    ('second', 3),
    ('shrink', 3, (0,)),
    ('shrink', 2, (1,)),
    ('shrink', 2, (3,)),
    ('shrink', 2, (2,)),
    ('third', 3),
    ('second', 2),
    ('second', 0),
    ('shrink', 2, (0,)),
    ('mix', 1),
    ('shrink', 0, (2,)),
    ('third', 2),
    ('third', 0),
    ('mix', 0),
    ('mix', 3),
    ('mix', 2),
)
PARTNERS = ((2, 1, 3), (3, 0, 2))
PICKS = (1, 0, 2, 3)
MIXES = (1, 0, 3, 2)


def layer_normed(tokens, norm_gain):
    values = tokens.astype(jnp.float32)
    center = values - jnp.mean(values, axis=-1, keepdims=True)
    spread = jnp.mean(center * center, axis=-1, keepdims=True)
    return (center * lax.rsqrt(spread + EPSILON) * norm_gain).astype(jnp.bfloat16)


def slot_numbers(chosen, experts):
    onehot = (chosen[..., None] == jnp.arange(experts, dtype=jnp.int32)).astype(jnp.int32)
    before = jnp.cumsum(onehot, axis=1) - onehot
    return jnp.sum(before * onehot, axis=-1)


def capacity_of(tok_rows, top_count, experts):
    return 2 * min(tok_rows // 2, 5 * tok_rows * top_count // (8 * experts))


def kernel(experts, cap, tokens_ref, gain_ref, ids_ref, weight_ref, wg_hbm, wu_hbm, wd_hbm,
           out_hbm, wgu, wdc, out_ref, normed, picks, routed, away, hid, chip, hop1, turn, hop2, final, back, total,
           load_sem, ws, wr, zs, zr, as_, ar, ams, amr, xs, xr, fs, fr, ds, dr, hs, hr,
           h1s, h1r, h2s, h2r, bs, br):
    ep, tp = lax.axis_index("ep"), lax.axis_index("tp")
    z, y = ep // HALVES, ep % HALVES
    x, c = tp // CORES, tp % CORES
    tok_rows, width = tokens_ref.shape
    quarter = out_ref.shape[1]
    units = wdc.shape[0] // CORES
    bf16, f32 = jnp.bfloat16, jnp.float32

    def columns_of(xx, cc):
        return pl.ds(pl.multiple_of((xx * CORES + cc) * quarter, quarter), quarter)

    def rows_of(yy):
        return pl.ds(pl.multiple_of(yy * cap, cap), cap)

    own_units, mate_units = pl.ds(0, units), pl.ds(units, units)
    loads = [
        pltpu.make_async_copy(wg_hbm.at[0], wgu.at[:, own_units], load_sem.at[0]),
        pltpu.make_async_copy(wu_hbm.at[0], wgu.at[:, mate_units], load_sem.at[1]),
    ] + [
        pltpu.make_async_copy(
            wd_hbm.at[0, :, columns_of(xx, c)], wdc.at[own_units, pl.ds(xx * quarter, quarter)], load_sem.at[2 + xx]
        )
        for xx in range(2)
    ]
    for load in loads:
        load.start()

    def device(zz, yy, xx, cc):
        return (zz * HALVES + yy, xx * CORES + cc)

    x_peer = device(z, y, 1 - x, c)
    y_peer = device(z, 1 - y, x, c)
    mate_peer = device(z, y, x, 1 - c)
    first = (z * HALVES + (c * (1 - y) + (1 - c) * y), (c * x + (1 - c) * (1 - x)) * CORES + c)
    second = (z * HALVES + (c * y + (1 - c) * (1 - y)), (c * (1 - x) + (1 - c) * x) * CORES + c)

    plane = [z] + [nearest(z, k, experts) for k in range(experts - 1)]

    barrier = pltpu.get_barrier_semaphore()
    peers = [x_peer, y_peer, mate_peer] + [device(p, y, x, c) for p in plane[1:]]
    for peer in peers:
        pl.semaphore_signal(barrier, inc=1, device_id=peer, device_id_type=MESH)

    ids = jnp.transpose(ids_ref[...])
    one, two = ids[:, 0:1], ids[:, 1:2]
    lane = lax.broadcasted_iota(jnp.int32, (tok_rows, 128), 1)
    places = lax.broadcasted_iota(jnp.int32, (tok_rows, cap), 1)
    expert = jnp.full((tok_rows, 128), -1, jnp.int32)
    for k, p in enumerate(plane):
        expert = jnp.where(lane == k, p, expert)
    named = jnp.logical_or(one == expert, two == expert)
    lower = (
        lax.broadcasted_iota(jnp.int32, (tok_rows, tok_rows), 1)
        < lax.broadcasted_iota(jnp.int32, (tok_rows, tok_rows), 0)
    )
    slot = jnp.dot(
        lower.astype(f32).astype(bf16), named.astype(f32).astype(bf16), preferred_element_type=f32
    )
    slot = jnp.where(named, slot, -1.0).astype(jnp.int32)

    values = tokens_ref[...].astype(f32)
    mean = jnp.mean(values, axis=-1, keepdims=True)
    center = values - mean
    spread = jnp.mean(center * center, axis=-1, keepdims=True)
    scale = lax.rsqrt(spread + EPSILON)

    def norm(columns):
        own = tokens_ref[:, columns].astype(f32) - mean
        normed[:, columns] = (own * scale * gain_ref[:, columns]).astype(bf16)

    def pick(k, columns):
        return lax.dot_general(
            picks[k], normed[:, columns], (((0,), (0,)), ((), ())), preferred_element_type=f32
        ).astype(bf16)

    mine = columns_of(x, c)
    norm(mine)

    sent = []

    def send(src, dst, send_sem, recv_sem, peer):
        copy = pltpu.make_async_remote_copy(
            src_ref=src, dst_ref=dst, send_sem=send_sem, recv_sem=recv_sem,
            device_id=peer, device_id_type=MESH,
        )
        copy.start()
        sent.append(copy)
        return copy

    def block(p, yy, xx, cc):
        return routed.at[plane[p], rows_of(yy), columns_of(xx, cc)]

    half = cap // 2

    def piece(yy, xx, i):
        return routed.at[z, pl.ds(pl.multiple_of(yy * cap + i * half, half), half), columns_of(xx, c)]

    here = routed.at[z, rows_of(y)]
    pl.semaphore_wait(barrier, len(peers))
    for k in PICKS:
        picks[k] = (places == slot[:, k:k + 1]).astype(f32).astype(bf16)
        if k:
            away[k - 1] = pick(k, mine)
            send(away.at[k - 1], routed.at[z, rows_of(y), mine], zs.at[k - 1], zr.at[z],
                 device(plane[k], y, x, c))
        else:
            here[:, mine] = pick(0, mine)
            for i in range(2):
                send(piece(y, x, i), piece(y, x, i), as_.at[i], ar.at[i], y_peer)
    norm(columns_of(1 - x, c))
    here[:, columns_of(1 - x, c)] = pick(0, columns_of(1 - x, c))
    b = piece(y, 1 - x, 1)
    send(b, b, as_.at[2], ar.at[2], y_peer)

    def hand_down():
        for xx in range(2):
            w_copies.append(send(
                wd_hbm.at[0, :, columns_of(xx, 1 - c)], wdc.at[mate_units, pl.ds(xx * quarter, quarter)],
                ws.at[xx], wr.at[xx], mate_peer))

    def arrived(dst, sem):
        pltpu.make_async_remote_copy(
            src_ref=dst, dst_ref=dst, send_sem=zs.at[0], recv_sem=sem,
            device_id=mate_peer, device_id_type=MESH,
        ).wait_recv()

    handed, ready, w_copies = {}, set(), []
    hop1_copies, hop2_copies = {}, {}

    def own_rest():
        for xx in (x, 1 - x):
            columns = columns_of(xx, 1 - c)
            norm(columns)
            here[:, columns] = pick(0, columns)

    def join(i):
        if i == 0:
            b = piece(1 - y, x, 0)
            arrived(b, ar.at[0])
            send(b, b, as_.at[3], ar.at[3], x_peer)
            send(b, b, ams.at[0], amr.at[0], mate_peer)
        else:
            b = piece(1 - y, x, 1)
            arrived(b, ar.at[1])
            send(b, b, ams.at[1], amr.at[1], mate_peer)
            arrived(piece(1 - y, 1 - x, 1), ar.at[2])
            arrived(piece(1 - y, 1 - x, 0), ar.at[3])
            b = block(0, 1 - y, 1 - x, c)
            send(b, b, ams.at[2], amr.at[2], mate_peer)

    def launch(p):
        b = block(p, y, x, c)
        arrived(b, zr.at[plane[p]])
        send(b, b, xs.at[p, 0], xr.at[p, 0], x_peer)
        send(b, b, xs.at[p, 1], xr.at[p, 1], y_peer)
        send(b, b, ds.at[p, 0], dr.at[p, 0], mate_peer)

    def relay(p):
        b = block(p, c * y + (1 - c) * (1 - y), c * (1 - x) + (1 - c) * x, c)
        arrived(b, xr.at[p, 1 - c])
        send(b, b, fs.at[p], fr.at[p], first)
        send(b, b, ds.at[p, 2 - c], dr.at[p, 2 - c], mate_peer)

    def share(p):
        b = block(p, (1 - c) * y + c * (1 - y), (1 - c) * (1 - x) + c * x, c)
        arrived(b, xr.at[p, c])
        send(b, b, ds.at[p, 1 + c], dr.at[p, 1 + c], mate_peer)

    def finish(p):
        b = block(p, 1 - y, 1 - x, c)
        arrived(b, fr.at[p])
        send(b, b, ds.at[p, 3], dr.at[p, 3], mate_peer)

    def expand(p, i):
        if p == 0 and i == 0:
            loads[0].wait()
            loads[1].wait()
        rows = rows_of(1 - y if i else y)
        if p == 0 and i == 1:
            for b in range(2):
                arrived(piece(1 - y, x, b), amr.at[b])
            arrived(block(0, 1 - y, 1 - x, 1 - c), amr.at[2])
        elif p and i == 0:
            arrived(block(p, y, x, 1 - c), dr.at[p, 0])
            arrived(block(p, y, 1 - x, 1 - c), dr.at[p, 1])
        elif p:
            arrived(block(p, 1 - y, x, 1 - c), dr.at[p, 2])
            arrived(block(p, 1 - y, 1 - x, 1 - c), dr.at[p, 3])
        both = jnp.dot(routed[plane[p], rows], wgu[...], preferred_element_type=f32)
        gate, up = both[:, :units], both[:, units:]
        hid[p, rows, own_units] = (gate / (1.0 + jnp.exp(-gate)) * up).astype(bf16)
        handed[p, i] = send(
            hid.at[p, rows, own_units], hid.at[p, rows, mate_units], hs.at[p, i], hr.at[p, i], mate_peer
        )

    def shrink(p, js):
        if not ready:
            for copy in loads[2:]:
                copy.wait()
            for copy in w_copies:
                copy.wait_recv()
        if p not in ready:
            ready.add(p)
            for i in range(2):
                handed[p, i].wait_recv()
        for j in js:
            low, high = j % 2, j // 2
            x_low, x_high = (1 - x if low else x), (1 - x if high else x)
            y_low, y_high = (1 - y if low else y), (1 - y if high else y)
            xx = c * x_low + (1 - c) * x_high
            yy = c * y_high + (1 - c) * y_low
            chip[p, j] = jnp.dot(
                hid[p, rows_of(yy)], wdc[:, pl.ds(pl.multiple_of(xx * quarter, quarter), quarter)],
                preferred_element_type=f32,
            ).astype(bf16)
            if j >= 2:
                hop1_copies[p, j - 2] = send(
                    chip.at[p, j], hop1.at[p, j - 2], h1s.at[p, j - 2], h1r.at[p, j - 2], first
                )

    def return_second(p):
        hop1_copies[p, 1].wait_recv()
        turn[p] = (chip[p, 1].astype(f32) + hop1[p, 1].astype(f32)).astype(bf16)
        hop2_copies[p] = send(turn.at[p], hop2.at[p], h2s.at[p], h2r.at[p], second)

    def return_third(p):
        hop1_copies[p, 0].wait_recv()
        part = chip[p, 0].astype(f32) + hop1[p, 0].astype(f32)
        hop2_copies[p].wait_recv()
        part = (part + hop2[p].astype(f32)).astype(bf16)
        if p == 0:
            back[z] = part
        else:
            final[p - 1] = part
            send(final.at[p - 1], back.at[z], bs.at[p - 1], br.at[z], device(plane[p], y, x, c))

    def mix(p):
        e = plane[p]
        if p:
            arrived(back.at[e], br.at[e])
        route = jnp.transpose(weight_ref[...])
        share = jnp.where(one == e, route[:, 0:1], 0.0) + jnp.where(two == e, route[:, 1:2], 0.0)
        value = share * jnp.dot(picks[p], back[e], preferred_element_type=f32)
        if p == MIXES[0]:
            total[...] = value
        elif p != MIXES[-1]:
            total[...] += value
        else:
            out_ref[...] = (total[...] + value).astype(bf16)

    steps = dict(wsend=hand_down, own_rest=own_rest, join=join, launch=launch, relay=relay, share=share, finish=finish, expand=expand,
                 shrink=shrink, second=return_second, third=return_third, mix=mix)
    for i, (name, *arguments) in enumerate(ORDER):
        if i == len(ORDER) - 1:
            for copy in sent[:-3]:
                copy.wait_send()
            del sent[:-3]
        steps[name](*arguments)

    store = pltpu.make_async_copy(out_ref, out_hbm, load_sem.at[4])
    store.start()
    for copy in sent:
        copy.wait_send()
    store.wait()


def nearest(z, k, experts):
    place = 0
    for zz in range(experts):
        near = zz if zz < experts - 1 - zz else experts - 1 - zz
        other = PARTNERS[near][k]
        place = place + jnp.where(z == zz, other if near == zz else experts - 1 - other, 0)
    return place


def fused_body(tokens, norm_gain, expert_ids, route_weight, w_gate, w_up, w_down):
    tok_rows, width = tokens.shape
    experts = lax.axis_size("ep") // HALVES
    cap = capacity_of(tok_rows, expert_ids.shape[1], experts)
    tp_count = lax.axis_size("tp")
    quarter = width // tp_count
    units = w_gate.shape[2]
    bf16 = jnp.bfloat16
    dma = pltpu.SemaphoreType.DMA
    vmem = pl.BlockSpec(memory_space=pltpu.VMEM)
    hbm = pl.BlockSpec(memory_space=pl.ANY)
    one, two = dma((experts,)), dma((experts, 2))
    return pl.pallas_call(
        functools.partial(kernel, experts, cap),
        out_shape=jax.ShapeDtypeStruct((tok_rows, quarter), bf16),
        in_specs=[vmem, vmem, vmem, vmem, hbm, hbm, hbm],
        out_specs=hbm,
        scratch_shapes=[
            pltpu.VMEM((width, 2 * units), bf16),
            pltpu.VMEM((CORES * units, 2 * quarter), bf16),
            pltpu.VMEM((tok_rows, quarter), bf16),
            pltpu.VMEM((tok_rows, width), bf16),
            pltpu.VMEM((experts, tok_rows, cap), bf16),
            pltpu.VMEM((experts, HALVES * cap, width), bf16),
            pltpu.VMEM((experts - 1, cap, quarter), bf16),
            pltpu.VMEM((experts, HALVES * cap, CORES * units), bf16),
            pltpu.VMEM((experts, 4, cap, quarter), bf16),
            pltpu.VMEM((experts, 2, cap, quarter), bf16),
            pltpu.VMEM((experts, cap, quarter), bf16),
            pltpu.VMEM((experts, cap, quarter), bf16),
            pltpu.VMEM((experts - 1, cap, quarter), bf16),
            pltpu.VMEM((experts, cap, quarter), bf16),
            pltpu.VMEM((tok_rows, quarter), jnp.float32),
            dma((5,)),
            dma((2,)), dma((2,)),
            one, one,
            dma((4,)), dma((4,)), dma((3,)), dma((3,)),
            two, two, one, one,
            dma((experts, 4)), dma((experts, 4)),
            two, two,
            two, two, one, one, one, one,
        ],
        compiler_params=pltpu.CompilerParams(
            collective_id=0, has_side_effects=True, vmem_limit_bytes=60 * 1024 * 1024
        ),
        name="expert_layer",
    )(tokens, norm_gain.reshape(1, -1), expert_ids.T, route_weight.T, w_gate, w_up, w_down)


def body(tokens, norm_gain, expert_ids, route_weight, w_gate, w_up, w_down):
    tok_rows, width = tokens.shape
    top_count = expert_ids.shape[1]
    ep_count = lax.axis_size("ep")
    experts = ep_count // HALVES
    capacity = capacity_of(tok_rows, top_count, experts)
    normed = layer_normed(tokens, norm_gain)
    padded = jnp.concatenate([normed, jnp.zeros((1, width), jnp.bfloat16)], axis=0)
    slots = slot_numbers(expert_ids.reshape(1, -1), experts).reshape(-1)
    flat_expert = expert_ids.reshape(-1)
    owner = jnp.arange(tok_rows * top_count, dtype=jnp.int32) // top_count
    place = flat_expert * capacity + slots
    table = jnp.full((experts * capacity,), tok_rows, jnp.int32).at[place].set(owner)
    outgoing = padded[table].reshape(experts, capacity, width)
    columns = width // lax.axis_size("tp")
    portion = lax.dynamic_slice_in_dim(outgoing, lax.axis_index("tp") * columns, columns, 2)
    doubled = jnp.repeat(portion, HALVES, axis=0)
    pieces = lax.all_to_all(doubled, "ep", split_axis=0, concat_axis=0, tiled=True)
    arrived = lax.all_gather(pieces, "tp", axis=2, tiled=True)
    routed = arrived.reshape(-1, width)
    gate = jnp.dot(routed, w_gate[0], preferred_element_type=jnp.float32)
    up = jnp.dot(routed, w_up[0], preferred_element_type=jnp.float32)
    hidden = (jax.nn.silu(gate) * up).astype(jnp.bfloat16)
    partial_value = jnp.dot(hidden, w_down[0], preferred_element_type=jnp.float32)
    reduced = lax.psum_scatter(
        partial_value.astype(jnp.bfloat16), "tp", scatter_dimension=1, tiled=True
    )
    returned = lax.all_to_all(
        reduced.reshape(ep_count, capacity, -1), "ep", split_axis=0, concat_axis=0, tiled=True
    )
    quarter = returned.shape[2]
    summed = returned.reshape(experts, HALVES, capacity, quarter).astype(jnp.float32).sum(axis=1)
    picked = summed.reshape(experts * capacity, quarter)[place].reshape(
        tok_rows, top_count, quarter
    )
    mixed = jnp.sum(route_weight[:, :, None] * picked, axis=1)
    return mixed.astype(jnp.bfloat16)


def choose(*args):
    tok_rows = args[0].shape[0]
    experts = lax.axis_size("ep") // HALVES
    cap = capacity_of(tok_rows, args[2].shape[1], experts)
    if experts == len(MIXES) and cap % 16 == 0 and lax.axis_size("tp") == 2 * CORES and args[2].shape[1] == 2:
        return fused_body(*args)
    return body(*args)


def solution(mesh):
    return jax.shard_map(
        choose,
        mesh=mesh,
        in_specs=(
            P("ep", None),
            P(),
            P("ep", None),
            P("ep", None),
            P("ep", None, "tp"),
            P("ep", None, "tp"),
            P("ep", "tp", None),
        ),
        out_specs=P("ep", "tp"),
        check_vma=False,
    )
```

```python
import functools

import jax
import jax.numpy as jnp
from jax import lax
from jax.experimental import pallas as pl
from jax.experimental.pallas import tpu as pltpu
from jax.sharding import PartitionSpec as P

HALVES = 2
CORES = 2
EPSILON = 1e-05
MESH = pl.DeviceIdType.MESH
ORDER = (
    ('join', 0),
    ('own_rest',),
    ('launch', 1),
    ('join', 1),
    ('wsend',),
    ('expand', 0, 0),
    ('launch', 2),
    ('expand', 0, 1),
    ('relay', 1),
    ('share', 1),
    ('expand', 1, 0),
    ('launch', 3),
    ('finish', 1),
    ('shrink', 0, (0,)),
    ('relay', 2),
    ('share', 2),
    ('expand', 1, 1),
    ('share', 3),
    ('relay', 3),
    ('shrink', 1, (3,)),
    ('shrink', 1, (2,)),
    ('expand', 3, 0),
    ('shrink', 1, (1,)),
    ('finish', 2),
    ('finish', 3),
    ('expand', 2, 0),
    ('second', 1),
    ('expand', 3, 1),
    ('shrink', 0, (3,)),
    ('shrink', 1, (0,)),
    ('shrink', 3, (3,)),
    ('third', 1),
    ('shrink', 3, (2,)),
    ('shrink', 3, (1,)),
    ('shrink', 0, (1,)),
    ('expand', 2, 1),
    ('second', 3),
    ('shrink', 3, (0,)),
    ('shrink', 2, (1,)),
    ('shrink', 2, (3,)),
    ('shrink', 2, (2,)),
    ('third', 3),
    ('second', 2),
    ('second', 0),
    ('shrink', 2, (0,)),
    ('mix', 1),
    ('shrink', 0, (2,)),
    ('third', 2),
    ('third', 0),
    ('mix', 0),
    ('mix', 3),
    ('mix', 2),
)
PARTNERS = ((2, 1, 3), (3, 0, 2))
PICKS = (1, 0, 2, 3)
HALF_FIRST = False
MIXES = (1, 0, 3, 2)


def layer_normed(tokens, norm_gain):
    values = tokens.astype(jnp.float32)
    center = values - jnp.mean(values, axis=-1, keepdims=True)
    spread = jnp.mean(center * center, axis=-1, keepdims=True)
    return (center * lax.rsqrt(spread + EPSILON) * norm_gain).astype(jnp.bfloat16)


def slot_numbers(chosen, experts):
    onehot = (chosen[..., None] == jnp.arange(experts, dtype=jnp.int32)).astype(jnp.int32)
    before = jnp.cumsum(onehot, axis=1) - onehot
    return jnp.sum(before * onehot, axis=-1)


def capacity_of(tok_rows, top_count, experts):
    return 2 * min(tok_rows // 2, 5 * tok_rows * top_count // (8 * experts))


def kernel(experts, cap, tokens_hbm, gain_hbm, ids_hbm, weight_hbm, wg_hbm, wu_hbm, wd_hbm,
           out_ref, tokens_ref, gain_ref, ids_ref, weight_ref, wgu, wdc, normed, spots, picks, shares, routed,
           away, hid, chip, hop1, turn, hop2, final, back, total, span,
           load_sem, sent_sem, wr, zr, ar, amr, xr, fr, dr, hr, h1r, h2r, br):
    ep, tp = lax.axis_index("ep"), lax.axis_index("tp")
    z, y = ep // HALVES, ep % HALVES
    x, c = tp // CORES, tp % CORES
    tok_rows, width = tokens_ref.shape
    quarter = out_ref.shape[1]
    units = wdc.shape[0] // CORES
    bf16, f32 = jnp.bfloat16, jnp.float32

    def columns_of(xx, cc):
        return pl.ds(pl.multiple_of((xx * CORES + cc) * quarter, quarter), quarter)

    def rows_of(yy):
        return pl.ds(pl.multiple_of(yy * cap, cap), cap)

    own_units, mate_units = pl.ds(0, units), pl.ds(units, units)
    inputs = [
        pltpu.make_async_copy(src, dst, load_sem.at[i])
        for i, (src, dst) in enumerate(
            ((tokens_hbm, tokens_ref), (ids_hbm, ids_ref), (gain_hbm, gain_ref), (weight_hbm, weight_ref)))
    ]
    for copy in inputs:
        copy.start()
    loads = [
        pltpu.make_async_copy(wg_hbm.at[0], wgu.at[:, own_units], load_sem.at[4]),
        pltpu.make_async_copy(wu_hbm.at[0], wgu.at[:, mate_units], load_sem.at[5]),
    ] + [
        pltpu.make_async_copy(
            wd_hbm.at[0, :, columns_of(xx, c)], wdc.at[own_units, pl.ds(xx * quarter, quarter)], load_sem.at[6 + xx]
        )
        for xx in range(2)
    ]

    def device(zz, yy, xx, cc):
        return (zz * HALVES + yy, xx * CORES + cc)

    x_peer = device(z, y, 1 - x, c)
    y_peer = device(z, 1 - y, x, c)
    mate_peer = device(z, y, x, 1 - c)
    first = (z * HALVES + (c * (1 - y) + (1 - c) * y), (c * x + (1 - c) * (1 - x)) * CORES + c)
    second = (z * HALVES + (c * y + (1 - c) * (1 - y)), (c * (1 - x) + (1 - c) * x) * CORES + c)

    plane = [z] + [nearest(z, k, experts) for k in range(experts - 1)]

    barrier = pltpu.get_barrier_semaphore()
    peers = [x_peer, y_peer, mate_peer] + [device(p, y, x, c) for p in plane[1:]]
    for peer in peers:
        pl.semaphore_signal(barrier, inc=1, device_id=peer, device_id_type=MESH)
    for load in loads:
        load.start()

    inputs[1].wait()
    kinds = 16
    index = lax.broadcasted_iota(jnp.int32, (kinds, tok_rows), 0)
    expert = jnp.full((kinds, tok_rows), -1, jnp.int32)
    for k, p in enumerate(plane):
        expert = jnp.where(index == k, p, expert)
    named = jnp.logical_or(ids_ref[0:1, :] == expert, ids_ref[1:2, :] == expert)
    earlier = (
        lax.broadcasted_iota(jnp.int32, (tok_rows, tok_rows), 0)
        < lax.broadcasted_iota(jnp.int32, (tok_rows, tok_rows), 1)
    )
    slot = jnp.dot(
        named.astype(f32).astype(bf16), earlier.astype(f32).astype(bf16), preferred_element_type=f32
    )
    slot = jnp.where(named, slot, -1.0)
    number = slot.astype(jnp.int32)
    places = lax.broadcasted_iota(jnp.int32, (cap, tok_rows), 0)
    for k in range(experts):
        spots[k] = (places == number[k:k + 1, :]).astype(f32).astype(bf16)

    for copy in (inputs[0], *inputs[2:]):
        copy.wait()
    values = tokens_ref[...].astype(f32)
    mean = jnp.mean(values, axis=-1, keepdims=True)
    center = values - mean
    spread = jnp.mean(center * center, axis=-1, keepdims=True)
    scale = lax.rsqrt(spread + EPSILON)

    def norm(columns):
        own = tokens_ref[:, columns].astype(f32) - mean
        normed[:, columns] = (own * scale * gain_ref[:, columns]).astype(bf16)

    def pick(k, columns):
        return jnp.dot(spots[k], normed[:, columns], preferred_element_type=f32).astype(bf16)

    mine = columns_of(x, c)
    norm(mine)

    sizes = [0, 0]

    def send(src, dst, recv_sem, peer, group=0):
        pltpu.make_async_remote_copy(
            src_ref=src, dst_ref=dst, send_sem=sent_sem.at[group], recv_sem=recv_sem,
            device_id=peer, device_id_type=MESH,
        ).start()
        sizes[group] += src.shape[0] * src.shape[1]

    def block(p, yy, xx, cc):
        return routed.at[plane[p], rows_of(yy), columns_of(xx, cc)]

    half = cap // 2

    def piece(yy, xx, i):
        return routed.at[z, pl.ds(pl.multiple_of(yy * cap + i * half, half), half), columns_of(xx, c)]

    here = routed.at[z, rows_of(y)]
    pl.semaphore_wait(barrier, len(peers))
    for k in PICKS:
        if k:
            away[k - 1] = pick(k, mine)
            send(away.at[k - 1], routed.at[z, rows_of(y), mine], zr.at[z], device(plane[k], y, x, c))
        else:
            here[:, mine] = pick(0, mine)
            for i in range(2):
                send(piece(y, x, i), piece(y, x, i), ar.at[i], y_peer)
    norm(columns_of(1 - x, c))
    here[:, columns_of(1 - x, c)] = pick(0, columns_of(1 - x, c))
    b = piece(y, 1 - x, 1)
    send(b, b, ar.at[2], y_peer)

    def hand_down():
        for xx in range(2):
            send(wd_hbm.at[0, :, columns_of(xx, 1 - c)], wdc.at[mate_units, pl.ds(xx * quarter, quarter)],
                 wr.at[0], mate_peer, 1)

    def arrived(dst, sem):
        pltpu.make_async_remote_copy(
            src_ref=dst, dst_ref=dst, send_sem=sent_sem.at[0], recv_sem=sem,
            device_id=mate_peer, device_id_type=MESH,
        ).wait_recv()

    ready = set()

    def own_rest():
        ids, route = jnp.transpose(ids_ref[...]), jnp.transpose(weight_ref[...])
        lane = lax.broadcasted_iota(jnp.int32, shares.shape, 1)
        expert = jnp.full(shares.shape, -1, jnp.int32)
        for k, p in enumerate(plane):
            expert = jnp.where(lane == k, p, expert)
        shares[...] = (
            jnp.where(ids[:, 0:1] == expert, route[:, 0:1], 0.0) + jnp.where(ids[:, 1:2] == expert, route[:, 1:2], 0.0)
        )
        number = jnp.transpose(slot).astype(jnp.int32)
        places = lax.broadcasted_iota(jnp.int32, (tok_rows, cap), 1)
        for k in range(experts):
            picks[k] = (places == number[:, k:k + 1]).astype(f32).astype(bf16)
        for xx in (x, 1 - x):
            columns = columns_of(xx, 1 - c)
            norm(columns)
            here[:, columns] = pick(0, columns)

    def join(i):
        if i == 0:
            b = piece(1 - y, x, 0)
            arrived(b, ar.at[0])
            send(b, b, ar.at[3], x_peer)
            send(b, b, amr.at[0], mate_peer)
        else:
            b = piece(1 - y, x, 1)
            arrived(b, ar.at[1])
            send(b, b, amr.at[0], mate_peer)
            arrived(piece(1 - y, 1 - x, 1), ar.at[2])
            arrived(piece(1 - y, 1 - x, 0), ar.at[3])
            b = block(0, 1 - y, 1 - x, c)
            send(b, b, amr.at[0], mate_peer)

    def launch(p):
        b = block(p, y, x, c)
        arrived(b, zr.at[plane[p]])
        send(b, b, xr.at[p - 1, 0], x_peer)
        send(b, b, xr.at[p - 1, 1], y_peer)
        send(b, b, dr.at[p - 1, 0], mate_peer)

    def relay(p):
        b = block(p, c * y + (1 - c) * (1 - y), c * (1 - x) + (1 - c) * x, c)
        arrived(b, xr.at[p - 1, 1 - c])
        send(b, b, fr.at[p - 1], first)
        send(b, b, dr.at[p - 1, 1 - c], mate_peer)

    def share(p):
        b = block(p, (1 - c) * y + c * (1 - y), (1 - c) * (1 - x) + c * x, c)
        arrived(b, xr.at[p - 1, c])
        send(b, b, dr.at[p - 1, c], mate_peer)

    def finish(p):
        b = block(p, 1 - y, 1 - x, c)
        arrived(b, fr.at[p - 1])
        send(b, b, dr.at[p - 1, 1], mate_peer)

    def expand(p, i):
        if p == 0 and i == 0:
            loads[0].wait()
            loads[1].wait()
        rows = rows_of(1 - y if i else y)
        if p == 0 and i == 1:
            arrived(routed.at[z, rows_of(1 - y), pl.ds(0, 2 * quarter)], amr.at[0])
        elif p:
            arrived(routed.at[plane[p], rows, pl.ds(0, 2 * quarter)], dr.at[p - 1, i])
        both = jnp.dot(routed[plane[p], rows], wgu[...], preferred_element_type=f32)
        gate, up = both[:, :units], both[:, units:]
        hid[p, rows, own_units] = (gate / (1.0 + jnp.exp(-gate)) * up).astype(bf16)
        send(hid.at[p, rows, own_units], hid.at[p, rows, mate_units], hr.at[p], mate_peer, 1)

    def shrink(p, js):
        if not ready:
            for copy in loads[2:]:
                copy.wait()
            arrived(wdc.at[mate_units], wr.at[0])
        if p not in ready:
            ready.add(p)
            arrived(hid.at[p, :, mate_units], hr.at[p])
        for j in js:
            low, high = j % 2, j // 2
            x_low, x_high = (1 - x if low else x), (1 - x if high else x)
            y_low, y_high = (1 - y if low else y), (1 - y if high else y)
            xx = c * x_low + (1 - c) * x_high
            yy = c * y_high + (1 - c) * y_low
            chip[p, j] = jnp.dot(
                hid[p, rows_of(yy)], wdc[:, pl.ds(pl.multiple_of(xx * quarter, quarter), quarter)],
                preferred_element_type=f32,
            ).astype(bf16)
            if j >= 2:
                send(chip.at[p, j], hop1.at[p, j - 2], h1r.at[p, j - 2], first, 1)

    def return_second(p):
        arrived(hop1.at[p, 1], h1r.at[p, 1])
        turn[p] = (chip[p, 1].astype(f32) + hop1[p, 1].astype(f32)).astype(bf16)
        send(turn.at[p], hop2.at[p], h2r.at[p], second, 1)

    def return_third(p):
        arrived(hop1.at[p, 0], h1r.at[p, 0])
        part = chip[p, 0].astype(f32) + hop1[p, 0].astype(f32)
        arrived(hop2.at[p], h2r.at[p])
        part = (part + hop2[p].astype(f32)).astype(bf16)
        if p == 0:
            back[z] = part
        else:
            final[p - 1] = part
            send(final.at[p - 1], back.at[z], br.at[z], device(plane[p], y, x, c), 1)

    def mix(p):
        e = plane[p]
        if p:
            arrived(back.at[e], br.at[e])
        value = shares[:, p:p + 1] * jnp.dot(picks[p], back[e], preferred_element_type=f32)
        if p == MIXES[0]:
            total[...] = value
        elif p != MIXES[-1]:
            total[...] += value
        else:
            out_ref[...] = (total[...] + value).astype(bf16)

    steps = dict(wsend=hand_down, own_rest=own_rest, join=join, launch=launch, relay=relay, share=share, finish=finish, expand=expand,
                 shrink=shrink, second=return_second, third=return_third, mix=mix)
    for i, (name, *arguments) in enumerate(ORDER):
        if i == len(ORDER) - 1:
            for g in range(2):
                whole = span.at[pl.ds(0, sizes[g] // quarter)]
                pltpu.make_async_copy(whole, whole, sent_sem.at[g]).wait()
        steps[name](*arguments)


def nearest(z, k, experts):
    place = 0
    for zz in range(experts):
        near = zz if zz < experts - 1 - zz else experts - 1 - zz
        other = PARTNERS[near][k]
        place = place + jnp.where(z == zz, other if near == zz else experts - 1 - other, 0)
    return place


def fused_body(tokens, norm_gain, expert_ids, route_weight, w_gate, w_up, w_down):
    tok_rows, width = tokens.shape
    experts = lax.axis_size("ep") // HALVES
    cap = capacity_of(tok_rows, expert_ids.shape[1], experts)
    tp_count = lax.axis_size("tp")
    quarter = width // tp_count
    units = w_gate.shape[2]
    bf16 = jnp.bfloat16
    dma = pltpu.SemaphoreType.DMA
    vmem = pl.BlockSpec(memory_space=pltpu.VMEM)
    hbm = pl.BlockSpec(memory_space=pl.ANY)
    rows = HALVES * cap
    return pl.pallas_call(
        functools.partial(kernel, experts, cap),
        out_shape=pltpu.VMEM((tok_rows, quarter), bf16),
        in_specs=[hbm] * 7,
        out_specs=vmem,
        scratch_shapes=[
            pltpu.VMEM(tokens.shape, bf16),
            pltpu.VMEM((1, width), jnp.float32),
            pltpu.VMEM(expert_ids.shape[::-1], jnp.int32),
            pltpu.VMEM(route_weight.shape[::-1], jnp.float32),
            pltpu.VMEM((width, 2 * units), bf16),
            pltpu.VMEM((CORES * units, 2 * quarter), bf16),
            pltpu.VMEM((tok_rows, width), bf16),
            pltpu.VMEM((experts, cap, tok_rows), bf16),
            pltpu.VMEM((experts, tok_rows, cap), bf16),
            pltpu.VMEM((tok_rows, 128), jnp.float32),
            pltpu.VMEM((experts, rows, width), bf16),
            pltpu.VMEM((experts - 1, cap, quarter), bf16),
            pltpu.VMEM((experts, rows, CORES * units), bf16),
            pltpu.VMEM((experts, 4, cap, quarter), bf16),
            pltpu.VMEM((experts, 2, cap, quarter), bf16),
            pltpu.VMEM((experts, cap, quarter), bf16),
            pltpu.VMEM((experts, cap, quarter), bf16),
            pltpu.VMEM((experts - 1, cap, quarter), bf16),
            pltpu.VMEM((experts, cap, quarter), bf16),
            pltpu.VMEM((tok_rows, quarter), jnp.float32),
            pltpu.VMEM((8 * experts * rows, quarter), bf16),
            dma((8,)), dma((2,)),
            dma((1,)), dma((experts,)), dma((4,)), dma((1,)),
            dma((experts - 1, 2)), dma((experts - 1,)), dma((experts - 1, 2)), dma((experts,)),
            dma((experts, 2)), dma((experts,)), dma((experts,)),
        ],
        compiler_params=pltpu.CompilerParams(
            collective_id=0, has_side_effects=True, vmem_limit_bytes=60 * 1024 * 1024
        ),
        name="expert_layer",
    )(tokens, norm_gain.reshape(1, -1), expert_ids.T, route_weight.T, w_gate, w_up, w_down)


def body(tokens, norm_gain, expert_ids, route_weight, w_gate, w_up, w_down):
    tok_rows, width = tokens.shape
    top_count = expert_ids.shape[1]
    ep_count = lax.axis_size("ep")
    experts = ep_count // HALVES
    capacity = capacity_of(tok_rows, top_count, experts)
    normed = layer_normed(tokens, norm_gain)
    padded = jnp.concatenate([normed, jnp.zeros((1, width), jnp.bfloat16)], axis=0)
    slots = slot_numbers(expert_ids.reshape(1, -1), experts).reshape(-1)
    flat_expert = expert_ids.reshape(-1)
    owner = jnp.arange(tok_rows * top_count, dtype=jnp.int32) // top_count
    place = flat_expert * capacity + slots
    table = jnp.full((experts * capacity,), tok_rows, jnp.int32).at[place].set(owner)
    outgoing = padded[table].reshape(experts, capacity, width)
    columns = width // lax.axis_size("tp")
    portion = lax.dynamic_slice_in_dim(outgoing, lax.axis_index("tp") * columns, columns, 2)
    doubled = jnp.repeat(portion, HALVES, axis=0)
    pieces = lax.all_to_all(doubled, "ep", split_axis=0, concat_axis=0, tiled=True)
    arrived = lax.all_gather(pieces, "tp", axis=2, tiled=True)
    routed = arrived.reshape(-1, width)
    gate = jnp.dot(routed, w_gate[0], preferred_element_type=jnp.float32)
    up = jnp.dot(routed, w_up[0], preferred_element_type=jnp.float32)
    hidden = (jax.nn.silu(gate) * up).astype(jnp.bfloat16)
    partial_value = jnp.dot(hidden, w_down[0], preferred_element_type=jnp.float32)
    reduced = lax.psum_scatter(
        partial_value.astype(jnp.bfloat16), "tp", scatter_dimension=1, tiled=True
    )
    returned = lax.all_to_all(
        reduced.reshape(ep_count, capacity, -1), "ep", split_axis=0, concat_axis=0, tiled=True
    )
    quarter = returned.shape[2]
    summed = returned.reshape(experts, HALVES, capacity, quarter).astype(jnp.float32).sum(axis=1)
    picked = summed.reshape(experts * capacity, quarter)[place].reshape(
        tok_rows, top_count, quarter
    )
    mixed = jnp.sum(route_weight[:, :, None] * picked, axis=1)
    return mixed.astype(jnp.bfloat16)


def choose(*args):
    tok_rows = args[0].shape[0]
    experts = lax.axis_size("ep") // HALVES
    cap = capacity_of(tok_rows, args[2].shape[1], experts)
    if experts == len(MIXES) and cap % 16 == 0 and lax.axis_size("tp") == 2 * CORES and args[2].shape[1] == 2:
        return fused_body(*args)
    return body(*args)


def solution(mesh):
    return jax.shard_map(
        choose,
        mesh=mesh,
        in_specs=(
            P("ep", None),
            P(),
            P("ep", None),
            P("ep", None),
            P("ep", None, "tp"),
            P("ep", None, "tp"),
            P("ep", "tp", None),
        ),
        out_specs=P("ep", "tp"),
        check_vma=False,
    )
```

```python
import functools

import jax
import jax.numpy as jnp
from jax import lax
from jax.experimental import pallas as pl
from jax.experimental.pallas import tpu as pltpu
from jax.sharding import PartitionSpec as P

HALVES = 2
CORES = 2
EPSILON = 1e-05
MESH = pl.DeviceIdType.MESH
ORDER = (
    ('own_rest',),
    ('join', 0),
    ('wsend',),
    ('dispatch', 1),
    ('launch', 1),
    ('expand', 0, 0),
    ('join', 1),
    ('dispatch', 3),
    ('launch', 2),
    ('expand', 0, 1),
    ('share', 1),
    ('relay', 1),
    ('expand', 1, 0),
    ('relay', 2),
    ('finish', 1),
    ('shrink', 0, (1,)),
    ('launch', 3),
    ('expand', 1, 1),
    ('shrink', 0, (0,)),
    ('share', 2),
    ('shrink', 1, (3,)),
    ('finish', 2),
    ('expand', 2, 0),
    ('relay', 3),
    ('expand', 2, 1),
    ('shrink', 1, (2,)),
    ('share', 3),
    ('shrink', 2, (3,)),
    ('shrink', 1, (1,)),
    ('shrink', 1, (0,)),
    ('shrink', 2, (1,)),
    ('second', 1),
    ('finish', 3),
    ('expand', 3, 0),
    ('shrink', 2, (2,)),
    ('expand', 3, 1),
    ('second', 2),
    ('third', 1),
    ('shrink', 3, (3,)),
    ('shrink', 3, (2,)),
    ('shrink', 2, (0,)),
    ('third', 2),
    ('shrink', 3, (1,)),
    ('second', 3),
    ('shrink', 3, (0,)),
    ('mix', 2),
    ('shrink', 0, (3,)),
    ('shrink', 0, (2,)),
    ('third', 3),
    ('second', 0),
    ('mix', 1),
    ('third', 0),
    ('mix', 0),
    ('mix', 3),
)
PARTNERS = ((2, 1, 3), (0, 3, 2))
PICKS = (2, 0)
HALF_FIRST = False
MIXES = (2, 1, 0, 3)


def layer_normed(tokens, norm_gain):
    values = tokens.astype(jnp.float32)
    center = values - jnp.mean(values, axis=-1, keepdims=True)
    spread = jnp.mean(center * center, axis=-1, keepdims=True)
    return (center * lax.rsqrt(spread + EPSILON) * norm_gain).astype(jnp.bfloat16)


def slot_numbers(chosen, experts):
    onehot = (chosen[..., None] == jnp.arange(experts, dtype=jnp.int32)).astype(jnp.int32)
    before = jnp.cumsum(onehot, axis=1) - onehot
    return jnp.sum(before * onehot, axis=-1)


def capacity_of(tok_rows, top_count, experts):
    return 2 * min(tok_rows // 2, 5 * tok_rows * top_count // (8 * experts))


def kernel(experts, cap, tokens_hbm, gain_hbm, ids_hbm, weight_hbm, wg_hbm, wu_hbm, wd_hbm,
           out_ref, tokens_ref, gain_ref, ids_ref, weight_ref, wgu, wdc, normed, spots, picks, shares, routed,
           away, hid, chip, hop1, turn, hop2, final, back, total, span,
           load_sem, sent_sem, wr, zr, ar, amr, xr, fr, dr, hr, h1r, h2r, br):
    ep, tp = lax.axis_index("ep"), lax.axis_index("tp")
    z, y = ep // HALVES, ep % HALVES
    x, c = tp // CORES, tp % CORES
    tok_rows, width = tokens_ref.shape
    quarter = out_ref.shape[1]
    units = wdc.shape[0] // CORES
    bf16, f32 = jnp.bfloat16, jnp.float32

    def columns_of(xx, cc):
        return pl.ds(pl.multiple_of((xx * CORES + cc) * quarter, quarter), quarter)

    def rows_of(yy):
        return pl.ds(pl.multiple_of(yy * cap, cap), cap)

    own_units, mate_units = pl.ds(0, units), pl.ds(units, units)
    inputs = [
        pltpu.make_async_copy(src, dst, load_sem.at[i])
        for i, (src, dst) in enumerate(
            ((tokens_hbm, tokens_ref), (ids_hbm, ids_ref), (gain_hbm, gain_ref), (weight_hbm, weight_ref)))
    ]
    for copy in inputs:
        copy.start()
    loads = [
        pltpu.make_async_copy(wg_hbm.at[0], wgu.at[:, own_units], load_sem.at[4]),
        pltpu.make_async_copy(wu_hbm.at[0], wgu.at[:, mate_units], load_sem.at[5]),
    ] + [
        pltpu.make_async_copy(
            wd_hbm.at[0, :, columns_of(xx, c)], wdc.at[own_units, pl.ds(xx * quarter, quarter)], load_sem.at[6 + xx]
        )
        for xx in range(2)
    ]

    def device(zz, yy, xx, cc):
        return (zz * HALVES + yy, xx * CORES + cc)

    x_peer = device(z, y, 1 - x, c)
    y_peer = device(z, 1 - y, x, c)
    mate_peer = device(z, y, x, 1 - c)
    first = (z * HALVES + (c * (1 - y) + (1 - c) * y), (c * x + (1 - c) * (1 - x)) * CORES + c)
    second = (z * HALVES + (c * y + (1 - c) * (1 - y)), (c * (1 - x) + (1 - c) * x) * CORES + c)

    plane = [z] + [nearest(z, k, experts) for k in range(experts - 1)]

    barrier = pltpu.get_barrier_semaphore()
    peers = [x_peer, y_peer, mate_peer] + [device(p, y, x, c) for p in plane[1:]]
    for peer in peers:
        pl.semaphore_signal(barrier, inc=1, device_id=peer, device_id_type=MESH)
    for load in loads:
        load.start()

    inputs[1].wait()
    kinds = 16
    index = lax.broadcasted_iota(jnp.int32, (kinds, tok_rows), 0)
    expert = jnp.full((kinds, tok_rows), -1, jnp.int32)
    for k, p in enumerate(plane):
        expert = jnp.where(index == k, p, expert)
    named = jnp.logical_or(ids_ref[0:1, :] == expert, ids_ref[1:2, :] == expert)
    earlier = (
        lax.broadcasted_iota(jnp.int32, (tok_rows, tok_rows), 0)
        < lax.broadcasted_iota(jnp.int32, (tok_rows, tok_rows), 1)
    )
    slot = jnp.dot(
        named.astype(f32).astype(bf16), earlier.astype(f32).astype(bf16), preferred_element_type=f32
    )
    slot = jnp.where(named, slot, -1.0)
    number = slot.astype(jnp.int32)
    places = lax.broadcasted_iota(jnp.int32, (cap, tok_rows), 0)
    for k in range(experts):
        spots[k] = (places == number[k:k + 1, :]).astype(f32).astype(bf16)

    for copy in (inputs[0], *inputs[2:]):
        copy.wait()
    values = tokens_ref[...].astype(f32)
    mean = jnp.mean(values, axis=-1, keepdims=True)
    center = values - mean
    spread = jnp.mean(center * center, axis=-1, keepdims=True)
    scale = lax.rsqrt(spread + EPSILON)

    def norm(columns):
        own = tokens_ref[:, columns].astype(f32) - mean
        normed[:, columns] = (own * scale * gain_ref[:, columns]).astype(bf16)

    def pick(k, columns):
        return jnp.dot(spots[k], normed[:, columns], preferred_element_type=f32).astype(bf16)

    mine = columns_of(x, c)
    norm(mine)

    sizes = [0, 0]

    def send(src, dst, recv_sem, peer, group=0):
        pltpu.make_async_remote_copy(
            src_ref=src, dst_ref=dst, send_sem=sent_sem.at[group], recv_sem=recv_sem,
            device_id=peer, device_id_type=MESH,
        ).start()
        sizes[group] += src.shape[0] * src.shape[1]

    def block(p, yy, xx, cc):
        return routed.at[plane[p], rows_of(yy), columns_of(xx, cc)]

    half = cap // 2

    def piece(yy, xx, i):
        return routed.at[z, pl.ds(pl.multiple_of(yy * cap + i * half, half), half), columns_of(xx, c)]

    def dispatch(k):
        away[k - 1] = pick(k, mine)
        send(away.at[k - 1], routed.at[z, rows_of(y), mine], zr.at[z], device(plane[k], y, x, c))

    here = routed.at[z, rows_of(y)]
    pl.semaphore_wait(barrier, len(peers))
    for k in PICKS:
        if k:
            dispatch(k)
        else:
            here[:, mine] = pick(0, mine)
            for i in range(2):
                send(piece(y, x, i), piece(y, x, i), ar.at[i], y_peer)
    norm(columns_of(1 - x, c))
    here[:, columns_of(1 - x, c)] = pick(0, columns_of(1 - x, c))
    b = piece(y, 1 - x, 1)
    send(b, b, ar.at[2], y_peer)

    def hand_down():
        for xx in range(2):
            send(wd_hbm.at[0, :, columns_of(xx, 1 - c)], wdc.at[mate_units, pl.ds(xx * quarter, quarter)],
                 wr.at[0], mate_peer, 1)

    def arrived(dst, sem):
        pltpu.make_async_remote_copy(
            src_ref=dst, dst_ref=dst, send_sem=sent_sem.at[0], recv_sem=sem,
            device_id=mate_peer, device_id_type=MESH,
        ).wait_recv()

    ready = set()

    def own_rest():
        ids, route = jnp.transpose(ids_ref[...]), jnp.transpose(weight_ref[...])
        lane = lax.broadcasted_iota(jnp.int32, shares.shape, 1)
        expert = jnp.full(shares.shape, -1, jnp.int32)
        for k, p in enumerate(plane):
            expert = jnp.where(lane == k, p, expert)
        shares[...] = (
            jnp.where(ids[:, 0:1] == expert, route[:, 0:1], 0.0) + jnp.where(ids[:, 1:2] == expert, route[:, 1:2], 0.0)
        )
        number = jnp.transpose(slot).astype(jnp.int32)
        places = lax.broadcasted_iota(jnp.int32, (tok_rows, cap), 1)
        for k in range(experts):
            picks[k] = (places == number[:, k:k + 1]).astype(f32).astype(bf16)
        for xx in (x, 1 - x):
            columns = columns_of(xx, 1 - c)
            norm(columns)
            here[:, columns] = pick(0, columns)

    def join(i):
        if i == 0:
            b = piece(1 - y, x, 0)
            arrived(b, ar.at[0])
            send(b, b, ar.at[3], x_peer)
            send(b, b, amr.at[0], mate_peer)
        else:
            b = piece(1 - y, x, 1)
            arrived(b, ar.at[1])
            send(b, b, amr.at[0], mate_peer)
            arrived(piece(1 - y, 1 - x, 1), ar.at[2])
            arrived(piece(1 - y, 1 - x, 0), ar.at[3])
            b = block(0, 1 - y, 1 - x, c)
            send(b, b, amr.at[0], mate_peer)

    def launch(p):
        b = block(p, y, x, c)
        arrived(b, zr.at[plane[p]])
        send(b, b, xr.at[p - 1, 0], x_peer)
        send(b, b, xr.at[p - 1, 1], y_peer)
        send(b, b, dr.at[p - 1, 0], mate_peer)

    def relay(p):
        b = block(p, c * y + (1 - c) * (1 - y), c * (1 - x) + (1 - c) * x, c)
        arrived(b, xr.at[p - 1, 1 - c])
        send(b, b, fr.at[p - 1], first)
        send(b, b, dr.at[p - 1, 1 - c], mate_peer)

    def share(p):
        b = block(p, (1 - c) * y + c * (1 - y), (1 - c) * (1 - x) + c * x, c)
        arrived(b, xr.at[p - 1, c])
        send(b, b, dr.at[p - 1, c], mate_peer)

    def finish(p):
        b = block(p, 1 - y, 1 - x, c)
        arrived(b, fr.at[p - 1])
        send(b, b, dr.at[p - 1, 1], mate_peer)

    def expand(p, i):
        if p == 0 and i == 0:
            loads[0].wait()
            loads[1].wait()
        rows = rows_of(1 - y if i else y)
        if p == 0 and i == 1:
            arrived(routed.at[z, rows_of(1 - y), pl.ds(0, 2 * quarter)], amr.at[0])
        elif p:
            arrived(routed.at[plane[p], rows, pl.ds(0, 2 * quarter)], dr.at[p - 1, i])
        both = jnp.dot(routed[plane[p], rows], wgu[...], preferred_element_type=f32)
        gate, up = both[:, :units], both[:, units:]
        hid[p, rows, own_units] = (gate / (1.0 + jnp.exp(-gate)) * up).astype(bf16)
        send(hid.at[p, rows, own_units], hid.at[p, rows, mate_units], hr.at[p], mate_peer, 1)

    def shrink(p, js):
        if not ready:
            for copy in loads[2:]:
                copy.wait()
            arrived(wdc.at[mate_units], wr.at[0])
        if p not in ready:
            ready.add(p)
            arrived(hid.at[p, :, mate_units], hr.at[p])
        for j in js:
            low, high = j % 2, j // 2
            x_low, x_high = (1 - x if low else x), (1 - x if high else x)
            y_low, y_high = (1 - y if low else y), (1 - y if high else y)
            xx = c * x_low + (1 - c) * x_high
            yy = c * y_high + (1 - c) * y_low
            chip[p, j] = jnp.dot(
                hid[p, rows_of(yy)], wdc[:, pl.ds(pl.multiple_of(xx * quarter, quarter), quarter)],
                preferred_element_type=f32,
            ).astype(bf16)
            if j >= 2:
                send(chip.at[p, j], hop1.at[p, j - 2], h1r.at[p, j - 2], first, 1)

    def return_second(p):
        arrived(hop1.at[p, 1], h1r.at[p, 1])
        turn[p] = (chip[p, 1].astype(f32) + hop1[p, 1].astype(f32)).astype(bf16)
        send(turn.at[p], hop2.at[p], h2r.at[p], second, 1)

    def return_third(p):
        arrived(hop1.at[p, 0], h1r.at[p, 0])
        part = chip[p, 0].astype(f32) + hop1[p, 0].astype(f32)
        arrived(hop2.at[p], h2r.at[p])
        part = (part + hop2[p].astype(f32)).astype(bf16)
        if p == 0:
            back[z] = part
        else:
            final[p - 1] = part
            send(final.at[p - 1], back.at[z], br.at[z], device(plane[p], y, x, c), 1)

    def mix(p):
        e = plane[p]
        if p:
            arrived(back.at[e], br.at[e])
        value = shares[:, p:p + 1] * jnp.dot(picks[p], back[e], preferred_element_type=f32)
        if p == MIXES[0]:
            total[...] = value
        elif p != MIXES[-1]:
            total[...] += value
        else:
            out_ref[...] = (total[...] + value).astype(bf16)

    steps = dict(dispatch=dispatch, wsend=hand_down, own_rest=own_rest, join=join, launch=launch, relay=relay, share=share, finish=finish, expand=expand,
                 shrink=shrink, second=return_second, third=return_third, mix=mix)
    for i, (name, *arguments) in enumerate(ORDER):
        if i == len(ORDER) - 1:
            for g in range(2):
                whole = span.at[pl.ds(0, sizes[g] // quarter)]
                pltpu.make_async_copy(whole, whole, sent_sem.at[g]).wait()
        steps[name](*arguments)


def nearest(z, k, experts):
    place = 0
    for zz in range(experts):
        near = zz if zz < experts - 1 - zz else experts - 1 - zz
        other = PARTNERS[near][k]
        place = place + jnp.where(z == zz, other if near == zz else experts - 1 - other, 0)
    return place


def fused_body(tokens, norm_gain, expert_ids, route_weight, w_gate, w_up, w_down):
    tok_rows, width = tokens.shape
    experts = lax.axis_size("ep") // HALVES
    cap = capacity_of(tok_rows, expert_ids.shape[1], experts)
    tp_count = lax.axis_size("tp")
    quarter = width // tp_count
    units = w_gate.shape[2]
    bf16 = jnp.bfloat16
    dma = pltpu.SemaphoreType.DMA
    vmem = pl.BlockSpec(memory_space=pltpu.VMEM)
    hbm = pl.BlockSpec(memory_space=pl.ANY)
    rows = HALVES * cap
    return pl.pallas_call(
        functools.partial(kernel, experts, cap),
        out_shape=pltpu.VMEM((tok_rows, quarter), bf16),
        in_specs=[hbm] * 7,
        out_specs=vmem,
        scratch_shapes=[
            pltpu.VMEM(tokens.shape, bf16),
            pltpu.VMEM((1, width), jnp.float32),
            pltpu.VMEM(expert_ids.shape[::-1], jnp.int32),
            pltpu.VMEM(route_weight.shape[::-1], jnp.float32),
            pltpu.VMEM((width, 2 * units), bf16),
            pltpu.VMEM((CORES * units, 2 * quarter), bf16),
            pltpu.VMEM((tok_rows, width), bf16),
            pltpu.VMEM((experts, cap, tok_rows), bf16),
            pltpu.VMEM((experts, tok_rows, cap), bf16),
            pltpu.VMEM((tok_rows, 128), jnp.float32),
            pltpu.VMEM((experts, rows, width), bf16),
            pltpu.VMEM((experts - 1, cap, quarter), bf16),
            pltpu.VMEM((experts, rows, CORES * units), bf16),
            pltpu.VMEM((experts, 4, cap, quarter), bf16),
            pltpu.VMEM((experts, 2, cap, quarter), bf16),
            pltpu.VMEM((experts, cap, quarter), bf16),
            pltpu.VMEM((experts, cap, quarter), bf16),
            pltpu.VMEM((experts - 1, cap, quarter), bf16),
            pltpu.VMEM((experts, cap, quarter), bf16),
            pltpu.VMEM((tok_rows, quarter), jnp.float32),
            pltpu.VMEM((8 * experts * rows, quarter), bf16),
            dma((8,)), dma((2,)),
            dma((1,)), dma((experts,)), dma((4,)), dma((1,)),
            dma((experts - 1, 2)), dma((experts - 1,)), dma((experts - 1, 2)), dma((experts,)),
            dma((experts, 2)), dma((experts,)), dma((experts,)),
        ],
        compiler_params=pltpu.CompilerParams(
            collective_id=0, has_side_effects=True, vmem_limit_bytes=60 * 1024 * 1024
        ),
        name="expert_layer",
    )(tokens, norm_gain.reshape(1, -1), expert_ids.T, route_weight.T, w_gate, w_up, w_down)


def body(tokens, norm_gain, expert_ids, route_weight, w_gate, w_up, w_down):
    tok_rows, width = tokens.shape
    top_count = expert_ids.shape[1]
    ep_count = lax.axis_size("ep")
    experts = ep_count // HALVES
    capacity = capacity_of(tok_rows, top_count, experts)
    normed = layer_normed(tokens, norm_gain)
    padded = jnp.concatenate([normed, jnp.zeros((1, width), jnp.bfloat16)], axis=0)
    slots = slot_numbers(expert_ids.reshape(1, -1), experts).reshape(-1)
    flat_expert = expert_ids.reshape(-1)
    owner = jnp.arange(tok_rows * top_count, dtype=jnp.int32) // top_count
    place = flat_expert * capacity + slots
    table = jnp.full((experts * capacity,), tok_rows, jnp.int32).at[place].set(owner)
    outgoing = padded[table].reshape(experts, capacity, width)
    columns = width // lax.axis_size("tp")
    portion = lax.dynamic_slice_in_dim(outgoing, lax.axis_index("tp") * columns, columns, 2)
    doubled = jnp.repeat(portion, HALVES, axis=0)
    pieces = lax.all_to_all(doubled, "ep", split_axis=0, concat_axis=0, tiled=True)
    arrived = lax.all_gather(pieces, "tp", axis=2, tiled=True)
    routed = arrived.reshape(-1, width)
    gate = jnp.dot(routed, w_gate[0], preferred_element_type=jnp.float32)
    up = jnp.dot(routed, w_up[0], preferred_element_type=jnp.float32)
    hidden = (jax.nn.silu(gate) * up).astype(jnp.bfloat16)
    partial_value = jnp.dot(hidden, w_down[0], preferred_element_type=jnp.float32)
    reduced = lax.psum_scatter(
        partial_value.astype(jnp.bfloat16), "tp", scatter_dimension=1, tiled=True
    )
    returned = lax.all_to_all(
        reduced.reshape(ep_count, capacity, -1), "ep", split_axis=0, concat_axis=0, tiled=True
    )
    quarter = returned.shape[2]
    summed = returned.reshape(experts, HALVES, capacity, quarter).astype(jnp.float32).sum(axis=1)
    picked = summed.reshape(experts * capacity, quarter)[place].reshape(
        tok_rows, top_count, quarter
    )
    mixed = jnp.sum(route_weight[:, :, None] * picked, axis=1)
    return mixed.astype(jnp.bfloat16)


def choose(*args):
    tok_rows = args[0].shape[0]
    experts = lax.axis_size("ep") // HALVES
    cap = capacity_of(tok_rows, args[2].shape[1], experts)
    if experts == len(MIXES) and cap % 16 == 0 and lax.axis_size("tp") == 2 * CORES and args[2].shape[1] == 2:
        return fused_body(*args)
    return body(*args)


def solution(mesh):
    return jax.shard_map(
        choose,
        mesh=mesh,
        in_specs=(
            P("ep", None),
            P(),
            P("ep", None),
            P("ep", None),
            P("ep", None, "tp"),
            P("ep", None, "tp"),
            P("ep", "tp", None),
        ),
        out_specs=P("ep", "tp"),
        check_vma=False,
    )
```

```python
import functools

import jax
import jax.numpy as jnp
from jax import lax
from jax.experimental import pallas as pl
from jax.experimental.pallas import tpu as pltpu
from jax.sharding import PartitionSpec as P

HALVES = 2
CORES = 2
EPSILON = 1e-05
MESH = pl.DeviceIdType.MESH
ORDER = (
    ('own_rest',),
    ('join', 0),
    ('wsend',),
    ('dispatch', 1),
    ('launch', 1),
    ('expand', 0, 0),
    ('join', 1),
    ('dispatch', 3),
    ('launch', 2),
    ('expand', 0, 1),
    ('share', 1),
    ('relay', 1),
    ('expand', 1, 0),
    ('relay', 2),
    ('finish', 1),
    ('shrink', 0, (1,)),
    ('launch', 3),
    ('expand', 1, 1),
    ('shrink', 0, (0,)),
    ('share', 2),
    ('shrink', 1, (3,)),
    ('finish', 2),
    ('expand', 2, 0),
    ('relay', 3),
    ('expand', 2, 1),
    ('shrink', 1, (2,)),
    ('share', 3),
    ('shrink', 2, (3,)),
    ('shrink', 1, (1,)),
    ('shrink', 1, (0,)),
    ('shrink', 2, (1,)),
    ('second', 1),
    ('finish', 3),
    ('expand', 3, 0),
    ('shrink', 2, (2,)),
    ('expand', 3, 1),
    ('second', 2),
    ('third', 1),
    ('shrink', 3, (3,)),
    ('shrink', 3, (2,)),
    ('shrink', 2, (0,)),
    ('third', 2),
    ('shrink', 3, (1,)),
    ('second', 3),
    ('shrink', 3, (0,)),
    ('mix', 2),
    ('shrink', 0, (3,)),
    ('shrink', 0, (2,)),
    ('third', 3),
    ('second', 0),
    ('mix', 1),
    ('third', 0),
    ('mix', 0),
    ('mix', 3),
)
PARTNERS = ((2, 1, 3), (0, 3, 2))
PICKS = (2, 0)
HALF_FIRST = False
MIXES = (2, 1, 0, 3)


def layer_normed(tokens, norm_gain):
    values = tokens.astype(jnp.float32)
    center = values - jnp.mean(values, axis=-1, keepdims=True)
    spread = jnp.mean(center * center, axis=-1, keepdims=True)
    return (center * lax.rsqrt(spread + EPSILON) * norm_gain).astype(jnp.bfloat16)


def slot_numbers(chosen, experts):
    onehot = (chosen[..., None] == jnp.arange(experts, dtype=jnp.int32)).astype(jnp.int32)
    before = jnp.cumsum(onehot, axis=1) - onehot
    return jnp.sum(before * onehot, axis=-1)


def capacity_of(tok_rows, top_count, experts):
    return 2 * min(tok_rows // 2, 5 * tok_rows * top_count // (8 * experts))


def kernel(experts, cap, tokens_hbm, gain_hbm, ids_hbm, weight_hbm, wg_hbm, wu_hbm, wd_hbm,
           out_ref, tokens_ref, gain_ref, ids_ref, weight_ref, wgu, wdc, normed, spots, picks, shares, routed,
           away, hid, chip, hop1, turn, hop2, final, back, total, span,
           load_sem, sent_sem, wr, zr, ar, amr, xr, fr, dr, hr, h1r, h2r, br):
    ep, tp = lax.axis_index("ep"), lax.axis_index("tp")
    z, y = ep // HALVES, ep % HALVES
    x, c = tp // CORES, tp % CORES
    tok_rows, width = tokens_ref.shape
    quarter = out_ref.shape[1]
    units = wdc.shape[0] // CORES
    bf16, f32 = jnp.bfloat16, jnp.float32

    def columns_of(xx, cc):
        return pl.ds(pl.multiple_of((xx * CORES + cc) * quarter, quarter), quarter)

    def rows_of(yy):
        return pl.ds(pl.multiple_of(yy * cap, cap), cap)

    own_units, mate_units = pl.ds(0, units), pl.ds(units, units)
    inputs = [
        pltpu.make_async_copy(src, dst, load_sem.at[i])
        for i, (src, dst) in enumerate(
            ((tokens_hbm, tokens_ref), (ids_hbm, ids_ref), (gain_hbm, gain_ref), (weight_hbm, weight_ref)))
    ]
    for copy in inputs:
        copy.start()
    loads = [
        pltpu.make_async_copy(wg_hbm.at[0], wgu.at[:, own_units], load_sem.at[4]),
        pltpu.make_async_copy(wu_hbm.at[0], wgu.at[:, mate_units], load_sem.at[5]),
    ] + [
        pltpu.make_async_copy(
            wd_hbm.at[0, :, columns_of(xx, c)], wdc.at[own_units, pl.ds(xx * quarter, quarter)], load_sem.at[6 + xx]
        )
        for xx in range(2)
    ]

    def device(zz, yy, xx, cc):
        return (zz * HALVES + yy, xx * CORES + cc)

    x_peer = device(z, y, 1 - x, c)
    y_peer = device(z, 1 - y, x, c)
    mate_peer = device(z, y, x, 1 - c)
    first = (z * HALVES + (c * (1 - y) + (1 - c) * y), (c * x + (1 - c) * (1 - x)) * CORES + c)
    second = (z * HALVES + (c * y + (1 - c) * (1 - y)), (c * (1 - x) + (1 - c) * x) * CORES + c)

    plane = [z] + [nearest(z, k, experts) for k in range(experts - 1)]

    barrier = pltpu.get_barrier_semaphore()
    peers = [x_peer, y_peer, mate_peer] + [device(p, y, x, c) for p in plane[1:]]
    for peer in peers:
        pl.semaphore_signal(barrier, inc=1, device_id=peer, device_id_type=MESH)
    for load in loads:
        load.start()

    with jax.named_scope("prep"):
        inputs[1].wait()
        kinds = 16
        index = lax.broadcasted_iota(jnp.int32, (kinds, tok_rows), 0)
        expert = jnp.full((kinds, tok_rows), -1, jnp.int32)
        for k, p in enumerate(plane):
            expert = jnp.where(index == k, p, expert)
        named = jnp.logical_or(ids_ref[0:1, :] == expert, ids_ref[1:2, :] == expert)
        earlier = (
            lax.broadcasted_iota(jnp.int32, (tok_rows, tok_rows), 0)
            < lax.broadcasted_iota(jnp.int32, (tok_rows, tok_rows), 1)
        )
        slot = jnp.dot(
            named.astype(f32).astype(bf16), earlier.astype(f32).astype(bf16), preferred_element_type=f32
        )
        slot = jnp.where(named, slot, -1.0)
        number = slot.astype(jnp.int32)
        places = lax.broadcasted_iota(jnp.int32, (cap, tok_rows), 0)
        for k in range(experts):
            spots[k] = (places == number[k:k + 1, :]).astype(f32).astype(bf16)

        for copy in (inputs[0], *inputs[2:]):
            copy.wait()
        values = tokens_ref[...].astype(f32)
        mean = jnp.mean(values, axis=-1, keepdims=True)
        center = values - mean
        spread = jnp.mean(center * center, axis=-1, keepdims=True)
        scale = lax.rsqrt(spread + EPSILON)

        def norm(columns):
            own = tokens_ref[:, columns].astype(f32) - mean
            normed[:, columns] = (own * scale * gain_ref[:, columns]).astype(bf16)

        def pick(k, columns):
            return jnp.dot(spots[k], normed[:, columns], preferred_element_type=f32).astype(bf16)

        mine = columns_of(x, c)
        norm(mine)

    sizes = [0, 0]

    def send(src, dst, recv_sem, peer, group=0):
        pltpu.make_async_remote_copy(
            src_ref=src, dst_ref=dst, send_sem=sent_sem.at[group], recv_sem=recv_sem,
            device_id=peer, device_id_type=MESH,
        ).start()
        sizes[group] += src.shape[0] * src.shape[1]

    def block(p, yy, xx, cc):
        return routed.at[plane[p], rows_of(yy), columns_of(xx, cc)]

    half = cap // 2

    def piece(yy, xx, i):
        return routed.at[z, pl.ds(pl.multiple_of(yy * cap + i * half, half), half), columns_of(xx, c)]

    def dispatch(k):
        away[k - 1] = pick(k, mine)
        send(away.at[k - 1], routed.at[z, rows_of(y), mine], zr.at[z], device(plane[k], y, x, c))

    here = routed.at[z, rows_of(y)]
    with jax.named_scope("barrier"):
        pl.semaphore_wait(barrier, len(peers))
    with jax.named_scope("picks"):
        for k in PICKS:
            if k:
                dispatch(k)
            else:
                here[:, mine] = pick(0, mine)
                for i in range(2):
                    send(piece(y, x, i), piece(y, x, i), ar.at[i], y_peer)
        norm(columns_of(1 - x, c))
        here[:, columns_of(1 - x, c)] = pick(0, columns_of(1 - x, c))
        b = piece(y, 1 - x, 1)
        send(b, b, ar.at[2], y_peer)

    def hand_down():
        for xx in range(2):
            send(wd_hbm.at[0, :, columns_of(xx, 1 - c)], wdc.at[mate_units, pl.ds(xx * quarter, quarter)],
                 wr.at[0], mate_peer, 1)

    def arrived(dst, sem):
        pltpu.make_async_remote_copy(
            src_ref=dst, dst_ref=dst, send_sem=sent_sem.at[0], recv_sem=sem,
            device_id=mate_peer, device_id_type=MESH,
        ).wait_recv()

    ready = set()

    def own_rest():
        ids, route = jnp.transpose(ids_ref[...]), jnp.transpose(weight_ref[...])
        lane = lax.broadcasted_iota(jnp.int32, shares.shape, 1)
        expert = jnp.full(shares.shape, -1, jnp.int32)
        for k, p in enumerate(plane):
            expert = jnp.where(lane == k, p, expert)
        shares[...] = (
            jnp.where(ids[:, 0:1] == expert, route[:, 0:1], 0.0) + jnp.where(ids[:, 1:2] == expert, route[:, 1:2], 0.0)
        )
        number = jnp.transpose(slot).astype(jnp.int32)
        places = lax.broadcasted_iota(jnp.int32, (tok_rows, cap), 1)
        for k in range(experts):
            picks[k] = (places == number[:, k:k + 1]).astype(f32).astype(bf16)
        for xx in (x, 1 - x):
            columns = columns_of(xx, 1 - c)
            norm(columns)
            here[:, columns] = pick(0, columns)

    def join(i):
        if i == 0:
            b = piece(1 - y, x, 0)
            arrived(b, ar.at[0])
            send(b, b, ar.at[3], x_peer)
            send(b, b, amr.at[0], mate_peer)
        else:
            b = piece(1 - y, x, 1)
            arrived(b, ar.at[1])
            send(b, b, amr.at[0], mate_peer)
            arrived(piece(1 - y, 1 - x, 1), ar.at[2])
            arrived(piece(1 - y, 1 - x, 0), ar.at[3])
            b = block(0, 1 - y, 1 - x, c)
            send(b, b, amr.at[0], mate_peer)

    def launch(p):
        b = block(p, y, x, c)
        arrived(b, zr.at[plane[p]])
        send(b, b, xr.at[p - 1, 0], x_peer)
        send(b, b, xr.at[p - 1, 1], y_peer)
        send(b, b, dr.at[p - 1, 0], mate_peer)

    def relay(p):
        b = block(p, c * y + (1 - c) * (1 - y), c * (1 - x) + (1 - c) * x, c)
        arrived(b, xr.at[p - 1, 1 - c])
        send(b, b, fr.at[p - 1], first)
        send(b, b, dr.at[p - 1, 1 - c], mate_peer)

    def share(p):
        b = block(p, (1 - c) * y + c * (1 - y), (1 - c) * (1 - x) + c * x, c)
        arrived(b, xr.at[p - 1, c])
        send(b, b, dr.at[p - 1, c], mate_peer)

    def finish(p):
        b = block(p, 1 - y, 1 - x, c)
        arrived(b, fr.at[p - 1])
        send(b, b, dr.at[p - 1, 1], mate_peer)

    def expand(p, i):
        if p == 0 and i == 0:
            loads[0].wait()
            loads[1].wait()
        rows = rows_of(1 - y if i else y)
        if p == 0 and i == 1:
            arrived(routed.at[z, rows_of(1 - y), pl.ds(0, 2 * quarter)], amr.at[0])
        elif p:
            arrived(routed.at[plane[p], rows, pl.ds(0, 2 * quarter)], dr.at[p - 1, i])
        both = jnp.dot(routed[plane[p], rows], wgu[...], preferred_element_type=f32)
        gate, up = both[:, :units], both[:, units:]
        hid[p, rows, own_units] = (gate / (1.0 + jnp.exp(-gate)) * up).astype(bf16)
        send(hid.at[p, rows, own_units], hid.at[p, rows, mate_units], hr.at[p], mate_peer, 1)

    def shrink(p, js):
        if not ready:
            for copy in loads[2:]:
                copy.wait()
            arrived(wdc.at[mate_units], wr.at[0])
        if p not in ready:
            ready.add(p)
            arrived(hid.at[p, :, mate_units], hr.at[p])
        for j in js:
            low, high = j % 2, j // 2
            x_low, x_high = (1 - x if low else x), (1 - x if high else x)
            y_low, y_high = (1 - y if low else y), (1 - y if high else y)
            xx = c * x_low + (1 - c) * x_high
            yy = c * y_high + (1 - c) * y_low
            chip[p, j] = jnp.dot(
                hid[p, rows_of(yy)], wdc[:, pl.ds(pl.multiple_of(xx * quarter, quarter), quarter)],
                preferred_element_type=f32,
            ).astype(bf16)
            if j >= 2:
                send(chip.at[p, j], hop1.at[p, j - 2], h1r.at[p, j - 2], first, 1)

    def return_second(p):
        arrived(hop1.at[p, 1], h1r.at[p, 1])
        turn[p] = (chip[p, 1].astype(f32) + hop1[p, 1].astype(f32)).astype(bf16)
        send(turn.at[p], hop2.at[p], h2r.at[p], second, 1)

    def return_third(p):
        arrived(hop1.at[p, 0], h1r.at[p, 0])
        part = chip[p, 0].astype(f32) + hop1[p, 0].astype(f32)
        arrived(hop2.at[p], h2r.at[p])
        part = (part + hop2[p].astype(f32)).astype(bf16)
        if p == 0:
            back[z] = part
        else:
            final[p - 1] = part
            send(final.at[p - 1], back.at[z], br.at[z], device(plane[p], y, x, c), 1)

    def mix(p):
        e = plane[p]
        if p:
            arrived(back.at[e], br.at[e])
        value = shares[:, p:p + 1] * jnp.dot(picks[p], back[e], preferred_element_type=f32)
        if p == MIXES[0]:
            total[...] = value
        elif p != MIXES[-1]:
            total[...] += value
        else:
            out_ref[...] = (total[...] + value).astype(bf16)

    steps = dict(dispatch=dispatch, wsend=hand_down, own_rest=own_rest, join=join, launch=launch, relay=relay, share=share, finish=finish, expand=expand,
                 shrink=shrink, second=return_second, third=return_third, mix=mix)
    for i, (name, *arguments) in enumerate(ORDER):
        if i == len(ORDER) - 1:
            for g in range(2):
                whole = span.at[pl.ds(0, sizes[g] // quarter)]
                pltpu.make_async_copy(whole, whole, sent_sem.at[g]).wait()
        with jax.named_scope(name + "".join(str(a).replace(" ", "") for a in arguments)):
            steps[name](*arguments)


def nearest(z, k, experts):
    place = 0
    for zz in range(experts):
        near = zz if zz < experts - 1 - zz else experts - 1 - zz
        other = PARTNERS[near][k]
        place = place + jnp.where(z == zz, other if near == zz else experts - 1 - other, 0)
    return place


def fused_body(tokens, norm_gain, expert_ids, route_weight, w_gate, w_up, w_down):
    tok_rows, width = tokens.shape
    experts = lax.axis_size("ep") // HALVES
    cap = capacity_of(tok_rows, expert_ids.shape[1], experts)
    tp_count = lax.axis_size("tp")
    quarter = width // tp_count
    units = w_gate.shape[2]
    bf16 = jnp.bfloat16
    dma = pltpu.SemaphoreType.DMA
    vmem = pl.BlockSpec(memory_space=pltpu.VMEM)
    hbm = pl.BlockSpec(memory_space=pl.ANY)
    rows = HALVES * cap
    return pl.pallas_call(
        functools.partial(kernel, experts, cap),
        out_shape=pltpu.VMEM((tok_rows, quarter), bf16),
        in_specs=[hbm] * 7,
        out_specs=vmem,
        scratch_shapes=[
            pltpu.VMEM(tokens.shape, bf16),
            pltpu.VMEM((1, width), jnp.float32),
            pltpu.VMEM(expert_ids.shape[::-1], jnp.int32),
            pltpu.VMEM(route_weight.shape[::-1], jnp.float32),
            pltpu.VMEM((width, 2 * units), bf16),
            pltpu.VMEM((CORES * units, 2 * quarter), bf16),
            pltpu.VMEM((tok_rows, width), bf16),
            pltpu.VMEM((experts, cap, tok_rows), bf16),
            pltpu.VMEM((experts, tok_rows, cap), bf16),
            pltpu.VMEM((tok_rows, 128), jnp.float32),
            pltpu.VMEM((experts, rows, width), bf16),
            pltpu.VMEM((experts - 1, cap, quarter), bf16),
            pltpu.VMEM((experts, rows, CORES * units), bf16),
            pltpu.VMEM((experts, 4, cap, quarter), bf16),
            pltpu.VMEM((experts, 2, cap, quarter), bf16),
            pltpu.VMEM((experts, cap, quarter), bf16),
            pltpu.VMEM((experts, cap, quarter), bf16),
            pltpu.VMEM((experts - 1, cap, quarter), bf16),
            pltpu.VMEM((experts, cap, quarter), bf16),
            pltpu.VMEM((tok_rows, quarter), jnp.float32),
            pltpu.VMEM((8 * experts * rows, quarter), bf16),
            dma((8,)), dma((2,)),
            dma((1,)), dma((experts,)), dma((4,)), dma((1,)),
            dma((experts - 1, 2)), dma((experts - 1,)), dma((experts - 1, 2)), dma((experts,)),
            dma((experts, 2)), dma((experts,)), dma((experts,)),
        ],
        compiler_params=pltpu.CompilerParams(
            collective_id=0, has_side_effects=True, vmem_limit_bytes=60 * 1024 * 1024
        ),
        name="expert_layer",
    )(tokens, norm_gain.reshape(1, -1), expert_ids.T, route_weight.T, w_gate, w_up, w_down)


def body(tokens, norm_gain, expert_ids, route_weight, w_gate, w_up, w_down):
    tok_rows, width = tokens.shape
    top_count = expert_ids.shape[1]
    ep_count = lax.axis_size("ep")
    experts = ep_count // HALVES
    capacity = capacity_of(tok_rows, top_count, experts)
    normed = layer_normed(tokens, norm_gain)
    padded = jnp.concatenate([normed, jnp.zeros((1, width), jnp.bfloat16)], axis=0)
    slots = slot_numbers(expert_ids.reshape(1, -1), experts).reshape(-1)
    flat_expert = expert_ids.reshape(-1)
    owner = jnp.arange(tok_rows * top_count, dtype=jnp.int32) // top_count
    place = flat_expert * capacity + slots
    table = jnp.full((experts * capacity,), tok_rows, jnp.int32).at[place].set(owner)
    outgoing = padded[table].reshape(experts, capacity, width)
    columns = width // lax.axis_size("tp")
    portion = lax.dynamic_slice_in_dim(outgoing, lax.axis_index("tp") * columns, columns, 2)
    doubled = jnp.repeat(portion, HALVES, axis=0)
    pieces = lax.all_to_all(doubled, "ep", split_axis=0, concat_axis=0, tiled=True)
    arrived = lax.all_gather(pieces, "tp", axis=2, tiled=True)
    routed = arrived.reshape(-1, width)
    gate = jnp.dot(routed, w_gate[0], preferred_element_type=jnp.float32)
    up = jnp.dot(routed, w_up[0], preferred_element_type=jnp.float32)
    hidden = (jax.nn.silu(gate) * up).astype(jnp.bfloat16)
    partial_value = jnp.dot(hidden, w_down[0], preferred_element_type=jnp.float32)
    reduced = lax.psum_scatter(
        partial_value.astype(jnp.bfloat16), "tp", scatter_dimension=1, tiled=True
    )
    returned = lax.all_to_all(
        reduced.reshape(ep_count, capacity, -1), "ep", split_axis=0, concat_axis=0, tiled=True
    )
    quarter = returned.shape[2]
    summed = returned.reshape(experts, HALVES, capacity, quarter).astype(jnp.float32).sum(axis=1)
    picked = summed.reshape(experts * capacity, quarter)[place].reshape(
        tok_rows, top_count, quarter
    )
    mixed = jnp.sum(route_weight[:, :, None] * picked, axis=1)
    return mixed.astype(jnp.bfloat16)


def choose(*args):
    tok_rows = args[0].shape[0]
    experts = lax.axis_size("ep") // HALVES
    cap = capacity_of(tok_rows, args[2].shape[1], experts)
    if experts == len(MIXES) and cap % 16 == 0 and lax.axis_size("tp") == 2 * CORES and args[2].shape[1] == 2:
        return fused_body(*args)
    return body(*args)


def solution(mesh):
    return jax.shard_map(
        choose,
        mesh=mesh,
        in_specs=(
            P("ep", None),
            P(),
            P("ep", None),
            P("ep", None),
            P("ep", None, "tp"),
            P("ep", None, "tp"),
            P("ep", "tp", None),
        ),
        out_specs=P("ep", "tp"),
        check_vma=False,
    )
```
